32 devices in a mesh: dp: 4 (over y, x), kv: 4 (over z), tp: 2 (over core).
Axes of the slice: x: 2, y: 2, z: 4, core: 2. Of those that a mesh axis runs over, the one named last changes fastest.
Arguments:
- tokens: bfloat16 [32, 2048], P('dp', ('kv', 'tp')), may hold values from -6 to 6
- gate_first: bfloat16 [2048, 5632], P(None, ('kv', 'tp')), may hold values from -0.110485435 to 0.110485435
- up_first: bfloat16 [2048, 5632], P(None, ('kv', 'tp')), may hold values from -0.110485435 to 0.110485435
- down_first: bfloat16 [5632, 2048], P(('kv', 'tp')), may hold values from -0.13325045 to 0.13325045
- gate_second: bfloat16 [2048, 5632], P(None, ('kv', 'tp')), may hold values from -0.110485435 to 0.110485435
- up_second: bfloat16 [2048, 5632], P(None, ('kv', 'tp')), may hold values from -0.110485435 to 0.110485435
- down_second: bfloat16 [5632, 2048], P(('kv', 'tp')), may hold values from -0.13325045 to 0.13325045
- query_weight: bfloat16 [2048, 1024], P('kv', 'tp'), may hold values from -0.125 to 0.125
- key_weight: bfloat16 [2048, 1024], P('kv', 'tp'), may hold values from -0.125 to 0.125
- value_weight: bfloat16 [2048, 1024], P('kv', 'tp'), may hold values from -0.125 to 0.125
- outgate_weight: bfloat16 [2048, 1024], P('kv', 'tp'), may hold values from -0.125 to 0.125
- decay_weight: bfloat16 [2048, 8], replicated, may hold values from -0.25 to 0.25
- write_weight: bfloat16 [2048, 8], replicated, may hold values from -0.25 to 0.25
- decay_rate: float32 [8], P('tp'), may hold values from -3 to 1
- norm_gain: float32 [128], replicated, may hold values from 0.1 to 1.9
- layer_gain: float32 [3, 2048], replicated, may hold values from 0.1 to 1.9
- out_weight: bfloat16 [1024, 2048], P('tp', 'kv'), may hold values from -0.375 to 0.375
- state: float32 [32, 8, 128, 128], P(('dp', 'kv'), 'tp'), may hold values from -0.6 to 0.6
Outputs:
- layer_out: bfloat16 [32, 2048], P('dp', ('kv', 'tp'))
- new_state: float32 [32, 8, 128, 128], P(('dp', 'kv'), 'tp')
The draws below stay inside these ranges and needn't reach their ends.
All inputs are finite; a program needn't handle non-finite values.
Results may differ from the reference program's by a relative error of at most 0.015.
Values may be sent and summed in bfloat16 or wider, within the bound.
A program may use at most 64 MiB of HBM per device.

```python
import jax
import jax.numpy as jnp
from jax import lax

D = 2048
FF = 5632
HEADS = 8
DK = 128
DV = 128
GROUP = 8
BATCH = 32
N_TP = 2


def normal_table(key, salted, dims):
    values = jax.random.normal(jax.random.fold_in(key, salted), dims, jnp.float32)
    return jnp.clip(values, -5.0, 5.0)


def draw_gate_first(key, part):
    return (normal_table(key, 11, (D, FF)) * D ** (-0.5)).astype(jnp.bfloat16)


def draw_up_first(key, part):
    jitter = normal_table(key, 12, (D, FF))
    values = jitter
    return (values * D ** (-0.5)).astype(jnp.bfloat16)


def draw_down_first(key, part):
    scaled = (FF // 4) ** (-0.5)
    values = normal_table(key, 13, (FF, D)) * scaled
    return values.astype(jnp.bfloat16)


def draw_gate_second(key, part):
    return (normal_table(key, 21, (D, FF)) * D ** (-0.5)).astype(jnp.bfloat16)


def draw_up_second(key, part):
    jitter = normal_table(key, 22, (D, FF))
    values = jitter
    return (values * D ** (-0.5)).astype(jnp.bfloat16)


def draw_down_second(key, part):
    scaled = (FF // 4) ** (-0.5)
    values = normal_table(key, 23, (FF, D)) * scaled
    return values.astype(jnp.bfloat16)


def block_levels(rng, extent, shards, least, largest):
    def one(position, shards_of):
        draws = jax.random.uniform(jax.random.fold_in(jax.random.fold_in(rng, 6), position), (shards_of,), jnp.float32, least / len(shards), largest / len(shards))
        return jnp.repeat(jnp.exp(draws), extent[position] // shards_of).reshape((-1,) + (1,) * (len(extent) - position - 1))

    factor_of = one(*shards[0])
    for cut in shards[1:]:
        factor_of = factor_of * one(*cut)
    return factor_of


def normal_values(own_key, shape, scale, bound, cuts=(), held_as=jnp.bfloat16):
    level = block_levels(own_key, shape, cuts, -0.22, 0.18) if cuts else 1.0
    array = jax.random.normal(own_key, shape, jnp.float32) * scale * level
    return jnp.minimum(jnp.maximum(array, -bound), bound).astype(held_as)


def setup_inputs(seed: int = 0) -> dict:
    streams_of = jax.random.split(jax.random.key(seed), 19)
    tokens = normal_values(streams_of[0], (BATCH, D), 1.0, 6.0, ((0, 4), (1, 8)))
    gate_first = draw_gate_first(jax.random.fold_in(streams_of[18], 71), 0)
    up_first = draw_up_first(jax.random.fold_in(streams_of[18], 71), 0)
    down_first = draw_down_first(jax.random.fold_in(streams_of[18], 71), 0)
    gate_second = draw_gate_second(jax.random.fold_in(streams_of[18], 71), 0)
    up_second = draw_up_second(jax.random.fold_in(streams_of[18], 71), 0)
    down_second = draw_down_second(jax.random.fold_in(streams_of[18], 71), 0)
    query_weight = normal_values(streams_of[7], (D, HEADS * DK), D ** -0.5, 0.125, ((0, 4), (1, 2)))
    key_weight = normal_values(streams_of[8], (D, HEADS * DK), D ** -0.5, 0.125, ((0, 4), (1, 2)))
    value_weight = normal_values(streams_of[9], (D, HEADS * DV), D ** -0.5, 0.125, ((0, 4), (1, 2)))
    outgate_weight = normal_values(streams_of[10], (D, HEADS * DV), D ** -0.5, 0.125, ((0, 4), (1, 2)))
    decay_weight = normal_values(streams_of[11], (D, HEADS), (D // 4) ** -0.5, 0.25)
    write_weight = normal_values(streams_of[12], (D, HEADS), (D // 4) ** -0.5, 0.25)
    decay_rate = jnp.clip(-3.0 + 4.0 * jax.random.uniform(streams_of[13], (HEADS,), jnp.float32) ** block_levels(streams_of[13], (HEADS,), ((0, 2),), -0.2, 0.2), -3.0, 1.0)
    norm_gain = jnp.clip(1.0 + 0.18 * jax.random.normal(streams_of[14], (DV,), jnp.float32), 0.1, 1.9)
    layer_gain = jnp.clip(1.0 + 0.18 * jax.random.normal(streams_of[15], (3, D), jnp.float32), 0.1, 1.9)
    out_weight = normal_values(streams_of[16], (HEADS * DV, D), (HEADS * DV // 4) ** -0.5, 0.375, ((0, 2), (1, 4)))
    state = normal_values(streams_of[17], (BATCH, HEADS, DK, DV), 0.1, 0.6, ((0, 16), (1, 2)), jnp.float32)
    return dict(tokens=tokens, gate_first=gate_first, up_first=up_first, down_first=down_first, gate_second=gate_second, up_second=up_second, down_second=down_second, query_weight=query_weight, key_weight=key_weight, value_weight=value_weight, outgate_weight=outgate_weight, decay_weight=decay_weight, write_weight=write_weight, decay_rate=decay_rate, norm_gain=norm_gain, layer_gain=layer_gain, out_weight=out_weight, state=state)


residual_scale = 2.0 ** 0.25
ln_eps = 1e-05
rms_eps = 1e-06

def layer_norm(rows, gain):
    values = rows.astype(jnp.float32)
    mean = lax.optimization_barrier(jnp.mean(values, -1, keepdims=True))
    spread = lax.optimization_barrier(jnp.mean(values * values, -1, keepdims=True)) - mean * mean
    return ((values - mean) * lax.rsqrt(spread + ln_eps) * gain).astype(jnp.bfloat16)

def feed_forward(rows, gate_w, up_w, down_w):
    gate = jnp.dot(rows, gate_w, preferred_element_type=jnp.float32)
    up = jnp.dot(rows, up_w, preferred_element_type=jnp.float32)
    hidden = (jax.nn.silu(gate) * up).astype(jnp.bfloat16)
    return jnp.dot(hidden, down_w, preferred_element_type=jnp.float32)

def unit_rows(values):
    return values * lax.rsqrt(lax.optimization_barrier(jnp.sum(values * values, -1, keepdims=True)) + rms_eps)

def state_block(inputs):
    query, keys, vals, beta, decay, old = inputs
    kept = old * jnp.exp(decay)[..., None, None]
    seen = jnp.einsum('bhk,bhkv->bhv', keys, kept, precision=lax.Precision.HIGHEST)
    delta = beta[..., None] * (vals - seen)
    fresh = kept + keys[..., :, None] * delta[..., None, :]
    outs = jnp.einsum('bhk,bhkv->bhv', query, fresh, precision=lax.Precision.HIGHEST)
    return (outs, fresh)

def reference(tokens, gate_first, up_first, down_first, gate_second, up_second, down_second, query_weight, key_weight, value_weight, outgate_weight, decay_weight, write_weight, decay_rate, norm_gain, layer_gain, out_weight, state):
    first = (residual_scale * tokens.astype(jnp.float32) + 0.5 * feed_forward(tokens, gate_first, up_first, down_first)).astype(jnp.bfloat16)
    first = lax.optimization_barrier(first)
    mixed_in = layer_norm(first, layer_gain[0])

    def project(weight):
        return jnp.dot(mixed_in, weight, preferred_element_type=jnp.float32).astype(jnp.bfloat16).astype(jnp.float32)
    query = jax.nn.silu(project(query_weight)).reshape(BATCH, HEADS, DK)
    query = unit_rows(query) * DK ** (-0.5)
    keys = unit_rows(jax.nn.silu(project(key_weight)).reshape(BATCH, HEADS, DK))
    vals = jax.nn.silu(project(value_weight)).reshape(BATCH, HEADS, DV)
    outgate = project(outgate_weight).reshape(BATCH, HEADS, DV)
    beta = jax.nn.sigmoid(project(write_weight))
    decay = -jnp.exp(decay_rate)[None, :] * jax.nn.softplus(project(decay_weight))
    blocks = BATCH // GROUP

    def split(values):
        return values.reshape((blocks, GROUP) + values.shape[1:])
    outs, fresh = lax.map(state_block, (split(query), split(keys), split(vals), split(beta), split(decay), split(state)))
    outs = outs.reshape(BATCH, HEADS, DV)
    new_state = fresh.reshape(BATCH, HEADS, DK, DV)
    normed = outs * lax.rsqrt(lax.optimization_barrier(jnp.mean(outs * outs, -1, keepdims=True)) + rms_eps) * norm_gain
    heads_out = (normed * jax.nn.silu(outgate)).astype(jnp.bfloat16).reshape(BATCH, HEADS * DV)
    half = HEADS * DV // N_TP
    mix = jnp.zeros((BATCH, D), jnp.float32)
    for group in range(N_TP):
        part = jnp.dot(heads_out[:, group * half:(group + 1) * half], out_weight[group * half:(group + 1) * half], preferred_element_type=jnp.float32).astype(jnp.bfloat16)
        part = lax.optimization_barrier(part)
        mix = mix + part.astype(jnp.float32)
    mix = mix.astype(jnp.bfloat16)
    second = (residual_scale * mixed_in.astype(jnp.float32) + mix.astype(jnp.float32)).astype(jnp.bfloat16)
    second = lax.optimization_barrier(second)
    mlp_in = layer_norm(second, layer_gain[1])
    third = (residual_scale * mlp_in.astype(jnp.float32) + 0.5 * feed_forward(mlp_in, gate_second, up_second, down_second)).astype(jnp.bfloat16)
    third = lax.optimization_barrier(third)
    layer_out = layer_norm(third, layer_gain[2])
    return (layer_out, new_state)
```

```python
import functools

import jax
import jax.numpy as jnp
from jax import lax
from jax.experimental import pallas as pl
from jax.experimental.pallas import tpu as pltpu
from jax.sharding import PartitionSpec as P

residual_scale = 2.0**0.25
ln_eps = 1e-05
rms_eps = 1e-06
f32 = jnp.float32
bf16 = jnp.bfloat16

TOK, RED1, GAINS, PAIR, STAT, PROJ, HEADS, MIX, ROWS2, RED2, STAT2 = range(11)


def finish_norm(values, total, squares, width, gain):
    mean = total[:, None] / width
    spread = squares[:, None] / width - mean * mean
    return ((values - mean) * lax.rsqrt(spread + ln_eps) * gain).astype(jnp.bfloat16)


def spread_norm(rows, gain, width):
    values = rows.astype(jnp.float32)
    total, squares = lax.psum((jnp.sum(values, -1), jnp.sum(values * values, -1)), ("kv", "tp"))
    return finish_norm(values, total, squares, width, gain)


def whole_norm(rows, gain):
    values = rows.astype(jnp.float32)
    return finish_norm(
        values, jnp.sum(values, -1), jnp.sum(values * values, -1), values.shape[1], gain
    )


def unit_rows(values):
    return values * lax.rsqrt(jnp.sum(values * values, -1, keepdims=True) + rms_eps)


def shards_by_collectives(
    tokens,
    gate_first,
    up_first,
    down_first,
    gate_second,
    up_second,
    down_second,
    query_weight,
    key_weight,
    value_weight,
    outgate_weight,
    decay_weight,
    write_weight,
    decay_rate,
    norm_gain,
    layer_gain,
    out_weight,
    state,
):
    kv_index = lax.axis_index("kv")
    tp_index = lax.axis_index("tp")
    width = decay_weight.shape[0]
    own = tokens.shape[1]
    block = query_weight.shape[0]
    local_heads = decay_rate.shape[0]
    key_size = state.shape[2]
    value_size = state.shape[3]
    seq_local = state.shape[0]
    own_start = (kv_index * lax.axis_size("tp") + tp_index) * own
    block_start = kv_index * block
    fold_piece = lax.all_gather(tokens, ("kv", "tp"), axis=1, tiled=True)
    gate = jnp.dot(fold_piece, gate_first, preferred_element_type=jnp.float32)
    up = jnp.dot(fold_piece, up_first, preferred_element_type=jnp.float32)
    hidden = (jax.nn.silu(gate) * up).astype(jnp.bfloat16)
    terms = jnp.dot(hidden, down_first, preferred_element_type=jnp.float32)
    branch = lax.psum_scatter(terms, ("kv", "tp"), scatter_dimension=1, tiled=True)
    first = (residual_scale * tokens.astype(jnp.float32) + 0.5 * branch).astype(jnp.bfloat16)
    first = lax.optimization_barrier(first)
    first_rows = lax.all_gather(first, ("kv", "tp"), axis=1, tiled=True)
    mixed_rows = whole_norm(first_rows, layer_gain[0])
    mixed_own = lax.dynamic_slice_in_dim(mixed_rows, own_start, own, 1)
    mixed_block = lax.dynamic_slice_in_dim(mixed_rows, block_start, block, 1)
    decay_part = lax.dynamic_slice(
        decay_weight, (block_start, tp_index * local_heads), (block, local_heads)
    )
    write_part = lax.dynamic_slice(
        write_weight, (block_start, tp_index * local_heads), (block, local_heads)
    )
    partials = tuple(
        (
            jnp.dot(mixed_block, weight, preferred_element_type=jnp.float32)
            for weight in (
                query_weight,
                key_weight,
                value_weight,
                outgate_weight,
                decay_part,
                write_part,
            )
        )
    )
    summed = lax.psum_scatter(partials, "kv", scatter_dimension=0, tiled=True)
    query_p, key_p, value_p, outgate_p, decay_p, write_p = tuple(
        (piece.astype(jnp.bfloat16).astype(jnp.float32) for piece in summed)
    )
    query = unit_rows(
        jax.nn.silu(query_p).reshape(seq_local, local_heads, key_size)
    ) * key_size ** (-0.5)
    keys = unit_rows(jax.nn.silu(key_p).reshape(seq_local, local_heads, key_size))
    vals = jax.nn.silu(value_p).reshape(seq_local, local_heads, value_size)
    outgate = outgate_p.reshape(seq_local, local_heads, value_size)
    beta = jax.nn.sigmoid(write_p)
    decay = -jnp.exp(decay_rate)[None, :] * jax.nn.softplus(decay_p)
    kept = state * jnp.exp(decay)[..., None, None]
    seen = jnp.einsum("bhk,bhkv->bhv", keys, kept, precision=lax.Precision.HIGHEST)
    delta = beta[..., None] * (vals - seen)
    new_state = kept + keys[..., :, None] * delta[..., None, :]
    outs = jnp.einsum("bhk,bhkv->bhv", query, new_state, precision=lax.Precision.HIGHEST)
    normed = outs * lax.rsqrt(jnp.mean(outs * outs, -1, keepdims=True) + rms_eps) * norm_gain
    heads_out = (
        (normed * jax.nn.silu(outgate))
        .astype(jnp.bfloat16)
        .reshape(seq_local, local_heads * value_size)
    )
    out_terms = jnp.dot(
        lax.all_gather(heads_out, "kv", axis=0, tiled=True),
        out_weight,
        preferred_element_type=jnp.float32,
    )
    mix = lax.psum_scatter(out_terms.astype(jnp.bfloat16), "tp", scatter_dimension=1, tiled=True)
    second = (residual_scale * mixed_own.astype(jnp.float32) + mix.astype(jnp.float32)).astype(
        jnp.bfloat16
    )
    second = lax.optimization_barrier(second)
    second_rows = lax.all_gather(second, ("kv", "tp"), axis=1, tiled=True)
    mlp_rows = whole_norm(second_rows, layer_gain[1])
    mlp_own = lax.dynamic_slice_in_dim(mlp_rows, own_start, own, 1)
    gate_two = jnp.dot(mlp_rows, gate_second, preferred_element_type=jnp.float32)
    up_two = jnp.dot(mlp_rows, up_second, preferred_element_type=jnp.float32)
    hidden_two = (jax.nn.silu(gate_two) * up_two).astype(jnp.bfloat16)
    terms_two = jnp.dot(hidden_two, down_second, preferred_element_type=jnp.float32)
    branch_two = lax.psum_scatter(terms_two, ("kv", "tp"), scatter_dimension=1, tiled=True)
    third = (residual_scale * mlp_own.astype(jnp.float32) + 0.5 * branch_two).astype(jnp.bfloat16)
    third = lax.optimization_barrier(third)
    gain_two = lax.dynamic_slice_in_dim(layer_gain[2], own_start, own)
    layer_out = spread_norm(third, gain_two, width)
    return (layer_out, new_state)


def dot(a, b):
    return jnp.dot(a, b, preferred_element_type=f32)


def silu(x):
    return x * jax.nn.sigmoid(x)


def kernel(
    n_kv,
    n_tp,
    tokens,
    gate_first,
    up_first,
    down_first,
    gate_second,
    up_second,
    down_second,
    query_weight,
    key_weight,
    value_weight,
    outgate_weight,
    decay_weight,
    write_weight,
    decay_rate,
    norm_gain,
    layer_gain,
    out_weight,
    state,
    layer_out,
    new_state,
    tok,
    g1,
    u1,
    d1,
    g2,
    u2,
    d2,
    wq,
    wk,
    wv,
    wo,
    wd,
    ww,
    rate,
    ngain,
    lgain,
    ow,
    st,
    ns,
    out_v,
    red_out,
    red_in,
    red_out2,
    red_in2,
    gain_buf,
    pair_buf,
    stat_buf,
    proj_out,
    proj_in,
    head_buf,
    mix_out,
    mix_in,
    rows_buf,
    stat2_buf,
    stat_rows,
    load_sem,
    send_sem,
    recv_sem,
):
    n = n_kv * n_tp
    kv = lax.axis_index("kv")
    tp = lax.axis_index("tp")
    me = kv * n_tp + tp
    group, own = tokens.shape
    width = n * own
    block = wq.shape[0]
    seqs, heads, dk, dv = state.shape
    pairs = seqs * heads
    cols = heads * dk
    own_start = pl.multiple_of(me * own, own)
    block_start = pl.multiple_of(kv * block, block)

    loads = {}

    def load(name, src, dst):
        loads[name] = pltpu.make_async_copy(src, dst, load_sem.at[len(loads)])
        loads[name].start()

    load("tok", tokens, tok.at[me])
    load("g1", gate_first, g1)
    load("u1", up_first, u1)
    load("d1", down_first, d1)
    load("lgain", layer_gain, lgain)
    load("wq", query_weight, wq)
    load("wk", key_weight, wk)
    load("wv", value_weight, wv)
    load("wo", outgate_weight, wo)
    load("wd", decay_weight.at[pl.ds(block_start, block)], wd)
    load("ww", write_weight.at[pl.ds(block_start, block)], ww)
    load("rate", decay_rate, rate)
    load("ngain", norm_gain, ngain)
    load("st", state, st)
    load("ow", out_weight, ow)
    load("g2", gate_second, g2)
    load("u2", up_second, u2)
    load("d2", down_second, d2)

    def peer_of(step):
        other = lax.rem(me + step, n)
        return other, lax.div(other, n_tp), lax.rem(other, n_tp)

    barrier = pltpu.get_barrier_semaphore()
    for step in range(1, n):
        _, pk, pt = peer_of(step)
        pl.semaphore_signal(
            barrier,
            inc=1,
            device_id={"kv": pk, "tp": pt},
            device_id_type=pl.DeviceIdType.MESH,
        )
    pl.semaphore_wait(barrier, n - 1)

    sends = []

    def send(kind, src, dst, pk, pt):
        other = pk * n_tp + pt
        copy = pltpu.make_async_remote_copy(
            src_ref=src,
            dst_ref=dst,
            send_sem=send_sem.at[kind, other],
            recv_sem=recv_sem.at[kind, me],
            device_id={"kv": pk, "tp": pt},
            device_id_type=pl.DeviceIdType.MESH,
        )
        copy.start()
        sends.append(copy)

    def receive(kind, dst, pk, pt):
        other = pk * n_tp + pt
        pltpu.make_async_remote_copy(
            src_ref=dst,
            dst_ref=dst,
            send_sem=send_sem.at[kind, other],
            recv_sem=recv_sem.at[kind, other],
            device_id={"kv": pk, "tp": pt},
            device_id_type=pl.DeviceIdType.MESH,
        ).wait_recv()

    def send_all(kind, src_of, dst):
        for step in range(1, n):
            other, pk, pt = peer_of(step)
            send(kind, src_of(other), dst, pk, pt)

    def receive_all(kind, buf):
        for step in range(1, n):
            other, pk, pt = peer_of(step)
            receive(kind, buf.at[other], pk, pt)

    def send_kv(kind, src_of, dst):
        for step in range(1, n_kv):
            pk = lax.rem(kv + step, n_kv)
            send(kind, src_of(pk), dst, pk, tp)

    def receive_kv(kind, buf):
        for step in range(1, n_kv):
            pk = lax.rem(kv + step, n_kv)
            receive(kind, buf.at[pk], pk, tp)

    other_tp = lax.rem(tp + 1, n_tp)

    loads["tok"].wait()
    send_all(TOK, lambda other: tok.at[me], tok.at[me])
    loads["g1"].wait()
    loads["u1"].wait()
    receive_all(TOK, tok)

    def feed_forward(rows, gw, uw, dw, wait_down, send_buf):
        x = jnp.concatenate(rows, axis=1)
        hidden = (silu(dot(x, gw[...])) * dot(x, uw[...])).astype(bf16)
        wait_down()
        terms = dot(hidden, dw[...]).astype(bf16)
        for part in range(n):
            send_buf[part] = terms[:, part * own : (part + 1) * own]

    feed_forward([tok[s] for s in range(n)], g1, u1, d1, loads["d1"].wait, red_out)
    send_all(RED1, lambda other: red_out.at[other], red_in.at[me])
    red_in[me] = red_out[me]

    for name in ("lgain", "wq", "wk", "wv", "wo", "wd", "ww"):
        loads[name].wait()
    gain_block = lgain[0:1, pl.ds(block_start, block)]

    def project(x):
        parts = [dot(x, w[...]) for w in (wq, wk, wv, wo)]
        for w in (wd, ww):
            parts.append(dot(x, w[...]))
        return parts

    n_small = wd.shape[1]
    spans = [i * cols for i in range(4)] + [4 * cols, 4 * cols + 128]
    lengths = [cols] * 4 + [n_small] * 2
    gains = project(jnp.broadcast_to(gain_block, (group, block)).astype(bf16))
    gain_buf[kv] = jnp.zeros(gain_buf.shape[1:], f32)
    for part, start, length in zip(gains, spans, lengths):
        gain_buf[kv, :, start : start + length] = part[0:1]
    send_kv(GAINS, lambda pk: gain_buf.at[kv], gain_buf.at[kv])

    receive_all(RED1, red_in)
    branch = red_in[0].astype(f32)
    for s in range(1, n):
        branch = branch + red_in[s].astype(f32)
    first = (residual_scale * tok[me].astype(f32) + 0.5 * branch).astype(bf16)
    pair_buf[tp] = first
    send(PAIR, pair_buf.at[tp], pair_buf.at[tp], kv, other_tp)
    first = first.astype(f32)

    def sums(values):
        lane = lax.broadcasted_iota(jnp.int32, (group, 128), 1)
        total = jnp.sum(values, -1, keepdims=True)
        squares = jnp.sum(values * values, -1, keepdims=True)
        return jnp.where(lane == 0, total, jnp.where(lane == 1, squares, 0.0))

    stat_buf[me] = sums(first)
    send_all(STAT, lambda other: stat_buf.at[me], stat_buf.at[me])
    receive(PAIR, pair_buf.at[other_tp], kv, other_tp)
    rows = jnp.concatenate([pair_buf[t].astype(f32) for t in range(n_tp)], axis=1)
    centre = jnp.sum(rows, -1, keepdims=True) / block
    partial = project(((rows - centre) * gain_block).astype(bf16))
    for j in range(n_kv):
        proj_out[j] = jnp.zeros(proj_out.shape[1:], bf16)
        for part, start, length in zip(partial, spans, lengths):
            proj_out[j, :, start : start + length] = part[
                j * seqs : (j + 1) * seqs
            ].astype(bf16)
    send_kv(PROJ, lambda pk: proj_out.at[pk], proj_in.at[kv])
    proj_in[kv] = proj_out[kv]

    receive_all(STAT, stat_buf)
    receive_kv(GAINS, gain_buf)

    def moments(buf):
        total = buf[0]
        for s in range(1, n):
            total = total + buf[s]
        mean = total[:, 0:1] / width
        spread = total[:, 1:2] / width - mean * mean
        return mean, lax.rsqrt(spread + ln_eps)

    mean, rstd = moments(stat_buf)
    own_gain = lgain[0:1, pl.ds(own_start, own)]
    mixed_own = ((first - mean) * rstd * own_gain).astype(bf16).astype(f32)
    lane = lax.broadcasted_iota(jnp.int32, (group, 128), 1)
    packed = jnp.where(lane == n_kv, rstd, 0.0)
    for j in range(n_kv):
        local = stat_buf[j * n_tp]
        for t in range(1, n_tp):
            local = local + stat_buf[j * n_tp + t]
        packed = jnp.where(lane == j, local[:, 0:1] / block - mean, packed)
    stat_rows[...] = packed
    mine = stat_rows[pl.ds(kv * seqs, seqs), :]

    receive_kv(PROJ, proj_in)
    summed = jnp.zeros((seqs, proj_in.shape[2]), f32)
    for j in range(n_kv):
        summed = summed + proj_in[j].astype(f32) + mine[:, j : j + 1] * gain_buf[j]
    summed = (summed * mine[:, n_kv : n_kv + 1]).astype(bf16).astype(f32)

    def by_head(base):
        return jnp.concatenate(
            [
                summed[s : s + 1, base + h * dk : base + (h + 1) * dk]
                for s in range(seqs)
                for h in range(heads)
            ],
            axis=0,
        )

    def unit(values):
        return values * lax.rsqrt(jnp.sum(values * values, -1, keepdims=True) + rms_eps)

    query = unit(silu(by_head(0))) * dk ** (-0.5)
    keys = unit(silu(by_head(cols)))
    vals = silu(by_head(2 * cols))
    outgate = by_head(3 * cols)
    pair_lane = lax.broadcasted_iota(jnp.int32, (pairs, 128), 1)
    pair_head = lax.rem(lax.broadcasted_iota(jnp.int32, (pairs, 128), 0), heads)

    def per_head(base):
        spread = jnp.concatenate(
            [
                jnp.broadcast_to(summed[s : s + 1, base : base + 128], (heads, 128))
                for s in range(seqs)
            ],
            axis=0,
        )
        picked = jnp.where(pair_lane == pair_head + tp * heads, spread, 0.0)
        return jnp.sum(picked, -1, keepdims=True)

    decay_pre = per_head(4 * cols)
    beta = jax.nn.sigmoid(per_head(4 * cols + 128))
    loads["rate"].wait()
    rate_lane = lax.broadcasted_iota(jnp.int32, (pairs, heads), 1)
    rate_head = lax.rem(lax.broadcasted_iota(jnp.int32, (pairs, heads), 0), heads)
    rates = jnp.sum(
        jnp.where(rate_lane == rate_head, jnp.broadcast_to(rate[...], (pairs, heads)), 0.0),
        -1,
        keepdims=True,
    )
    softplus = jnp.maximum(decay_pre, 0.0) + jnp.log1p(jnp.exp(-jnp.abs(decay_pre)))
    factor = jnp.broadcast_to(jnp.exp(-jnp.exp(rates) * softplus), (pairs, dv))
    beta = jnp.broadcast_to(beta, (pairs, dv))
    keys_t = jnp.transpose(keys)
    query_t = jnp.transpose(query)
    loads["st"].wait()
    outs = []
    for s in range(seqs):
        for h in range(heads):
            i = s * heads + h
            kept = st[s, h] * factor[i : i + 1]
            key = keys_t[:, i : i + 1]
            seen = jnp.sum(kept * key, 0, keepdims=True)
            fresh = kept + key * (beta[i : i + 1] * (vals[i : i + 1] - seen))
            ns[s, h] = fresh
            outs.append(jnp.sum(fresh * query_t[:, i : i + 1], 0, keepdims=True))
    outs = jnp.concatenate(outs, axis=0)
    loads["ngain"].wait()
    normed = outs * lax.rsqrt(jnp.mean(outs * outs, -1, keepdims=True) + rms_eps) * ngain[...]
    gated = (normed * silu(outgate)).astype(bf16)
    for s in range(seqs):
        for h in range(heads):
            i = s * heads + h
            head_buf[kv, s : s + 1, h * dv : (h + 1) * dv] = gated[i : i + 1]
    send_kv(HEADS, lambda pk: head_buf.at[kv], head_buf.at[kv])
    store = pltpu.make_async_copy(ns, new_state, load_sem.at[len(loads)])
    store.start()
    loads["ow"].wait()
    receive_kv(HEADS, head_buf)
    everyone = jnp.concatenate([head_buf[j].astype(f32) for j in range(n_kv)], axis=0)
    terms = dot(everyone.astype(bf16), ow[...]).astype(bf16)
    for t in range(n_tp):
        mix_out[t] = terms[:, t * own : (t + 1) * own]
    send(MIX, mix_out.at[other_tp], mix_in, kv, other_tp)
    kept_half = mix_out[tp].astype(f32)
    receive(MIX, mix_in, kv, other_tp)
    mix = (kept_half + mix_in[...].astype(f32)).astype(bf16).astype(f32)
    rows_buf[me] = (residual_scale * mixed_own + mix).astype(bf16)
    send_all(ROWS2, lambda other: rows_buf.at[me], rows_buf.at[me])
    loads["g2"].wait()
    loads["u2"].wait()
    receive_all(ROWS2, rows_buf)

    second = [rows_buf[s].astype(f32) for s in range(n)]
    total = sum(jnp.sum(v, -1, keepdims=True) for v in second)
    squares = sum(jnp.sum(v * v, -1, keepdims=True) for v in second)
    mean = total / width
    rstd = lax.rsqrt(squares / width - mean * mean + ln_eps)

    def normalise(v, start):
        return ((v - mean) * rstd * lgain[1:2, pl.ds(start, own)]).astype(bf16)

    mlp_own = normalise(rows_buf[me].astype(f32), own_start).astype(f32)
    feed_forward(
        [normalise(v, s * own) for s, v in enumerate(second)],
        g2,
        u2,
        d2,
        loads["d2"].wait,
        red_out2,
    )
    send_all(RED2, lambda other: red_out2.at[other], red_in2.at[me])
    red_in2[me] = red_out2[me]
    receive_all(RED2, red_in2)
    branch = red_in2[0].astype(f32)
    for s in range(1, n):
        branch = branch + red_in2[s].astype(f32)
    third = (residual_scale * mlp_own + 0.5 * branch).astype(bf16).astype(f32)
    stat2_buf[me] = sums(third)
    send_all(STAT2, lambda other: stat2_buf.at[me], stat2_buf.at[me])
    receive_all(STAT2, stat2_buf)
    mean, rstd = moments(stat2_buf)
    out_v[...] = ((third - mean) * rstd * lgain[2:3, pl.ds(own_start, own)]).astype(bf16)
    final = pltpu.make_async_copy(out_v, layer_out, load_sem.at[len(loads) + 1])
    final.start()
    for copy in sends:
        copy.wait_send()
    store.wait()
    final.wait()


def shards(n_kv, n_tp, *args):
    if args[0].shape[1] % 128 or args[17].shape[2] != 128:
        return shards_by_collectives(*args)
    args = list(args)
    args[13] = args[13].reshape(1, -1)
    args[14] = args[14].reshape(1, -1)
    tokens, decay_weight, state = args[0], args[11], args[17]
    query_weight = args[7]
    n = n_kv * n_tp
    group, own = tokens.shape
    seqs = state.shape[0]
    block, cols = query_weight.shape
    small = decay_weight.shape[1]
    flat = 4 * cols + 2 * 128

    def like(x):
        return pltpu.VMEM(x.shape, x.dtype)

    scratch = [
        pltpu.VMEM((n, group, own), bf16),
        *[like(x) for x in args[1:11]],
        pltpu.VMEM((block, small), bf16),
        pltpu.VMEM((block, small), bf16),
        *[like(x) for x in args[13:18]],
        like(state),
        like(tokens),
        pltpu.VMEM((n, group, own), bf16),
        pltpu.VMEM((n, group, own), bf16),
        pltpu.VMEM((n, group, own), bf16),
        pltpu.VMEM((n, group, own), bf16),
        pltpu.VMEM((n_kv, 1, flat), f32),
        pltpu.VMEM((n_tp, group, own), bf16),
        pltpu.VMEM((n, group, 128), f32),
        pltpu.VMEM((n_kv, seqs, flat), bf16),
        pltpu.VMEM((n_kv, seqs, flat), bf16),
        pltpu.VMEM((n_kv, seqs, cols), bf16),
        pltpu.VMEM((n_tp, group, own), bf16),
        pltpu.VMEM((group, own), bf16),
        pltpu.VMEM((n, group, own), bf16),
        pltpu.VMEM((n, group, 128), f32),
        pltpu.VMEM((group, 128), f32),
        pltpu.SemaphoreType.DMA((20,)),
        pltpu.SemaphoreType.DMA((11, n)),
        pltpu.SemaphoreType.DMA((11, n)),
    ]
    return pl.pallas_call(
        functools.partial(kernel, n_kv, n_tp),
        out_shape=(
            jax.ShapeDtypeStruct(tokens.shape, tokens.dtype),
            jax.ShapeDtypeStruct(state.shape, state.dtype),
        ),
        in_specs=[pl.BlockSpec(memory_space=pl.ANY)] * len(args),
        out_specs=(pl.BlockSpec(memory_space=pl.ANY),) * 2,
        scratch_shapes=scratch,
        compiler_params=pltpu.CompilerParams(
            collective_id=0, has_side_effects=True, vmem_limit_bytes=60 * 1024 * 1024
        ),
    )(*args)


def solution(mesh):
    in_specs = (
        P("dp", ("kv", "tp")),
        P(None, ("kv", "tp")),
        P(None, ("kv", "tp")),
        P(("kv", "tp"), None),
        P(None, ("kv", "tp")),
        P(None, ("kv", "tp")),
        P(("kv", "tp"), None),
        P("kv", "tp"),
        P("kv", "tp"),
        P("kv", "tp"),
        P("kv", "tp"),
        P(),
        P(),
        P("tp"),
        P(),
        P(),
        P("tp", "kv"),
        P(("dp", "kv"), "tp", None, None),
    )
    out_specs = (P("dp", ("kv", "tp")), P(("dp", "kv"), "tp", None, None))
    body = functools.partial(shards, mesh.shape["kv"], mesh.shape["tp"])
    return jax.shard_map(body, mesh=mesh, in_specs=in_specs, out_specs=out_specs, check_vma=False)
```

```python
import functools

import jax
import jax.numpy as jnp
from jax import lax
from jax.experimental import pallas as pl
from jax.experimental.pallas import tpu as pltpu
from jax.sharding import PartitionSpec as P

residual_scale = 2.0**0.25
ln_eps = 1e-05
rms_eps = 1e-06
f32 = jnp.float32
bf16 = jnp.bfloat16

TOK, RED1, GAINS, PAIR, STAT, PROJ, HEADS, MIX, ROWS2, RED2, STAT2 = range(11)


def finish_norm(values, total, squares, width, gain):
    mean = total[:, None] / width
    spread = squares[:, None] / width - mean * mean
    return ((values - mean) * lax.rsqrt(spread + ln_eps) * gain).astype(jnp.bfloat16)


def spread_norm(rows, gain, width):
    values = rows.astype(jnp.float32)
    total, squares = lax.psum((jnp.sum(values, -1), jnp.sum(values * values, -1)), ("kv", "tp"))
    return finish_norm(values, total, squares, width, gain)


def whole_norm(rows, gain):
    values = rows.astype(jnp.float32)
    return finish_norm(
        values, jnp.sum(values, -1), jnp.sum(values * values, -1), values.shape[1], gain
    )


def unit_rows(values):
    return values * lax.rsqrt(jnp.sum(values * values, -1, keepdims=True) + rms_eps)


def shards_by_collectives(
    tokens,
    gate_first,
    up_first,
    down_first,
    gate_second,
    up_second,
    down_second,
    query_weight,
    key_weight,
    value_weight,
    outgate_weight,
    decay_weight,
    write_weight,
    decay_rate,
    norm_gain,
    layer_gain,
    out_weight,
    state,
):
    kv_index = lax.axis_index("kv")
    tp_index = lax.axis_index("tp")
    width = decay_weight.shape[0]
    own = tokens.shape[1]
    block = query_weight.shape[0]
    local_heads = decay_rate.shape[0]
    key_size = state.shape[2]
    value_size = state.shape[3]
    seq_local = state.shape[0]
    own_start = (kv_index * lax.axis_size("tp") + tp_index) * own
    block_start = kv_index * block
    fold_piece = lax.all_gather(tokens, ("kv", "tp"), axis=1, tiled=True)
    gate = jnp.dot(fold_piece, gate_first, preferred_element_type=jnp.float32)
    up = jnp.dot(fold_piece, up_first, preferred_element_type=jnp.float32)
    hidden = (jax.nn.silu(gate) * up).astype(jnp.bfloat16)
    terms = jnp.dot(hidden, down_first, preferred_element_type=jnp.float32)
    branch = lax.psum_scatter(terms, ("kv", "tp"), scatter_dimension=1, tiled=True)
    first = (residual_scale * tokens.astype(jnp.float32) + 0.5 * branch).astype(jnp.bfloat16)
    first = lax.optimization_barrier(first)
    first_rows = lax.all_gather(first, ("kv", "tp"), axis=1, tiled=True)
    mixed_rows = whole_norm(first_rows, layer_gain[0])
    mixed_own = lax.dynamic_slice_in_dim(mixed_rows, own_start, own, 1)
    mixed_block = lax.dynamic_slice_in_dim(mixed_rows, block_start, block, 1)
    decay_part = lax.dynamic_slice(
        decay_weight, (block_start, tp_index * local_heads), (block, local_heads)
    )
    write_part = lax.dynamic_slice(
        write_weight, (block_start, tp_index * local_heads), (block, local_heads)
    )
    partials = tuple(
        (
            jnp.dot(mixed_block, weight, preferred_element_type=jnp.float32)
            for weight in (
                query_weight,
                key_weight,
                value_weight,
                outgate_weight,
                decay_part,
                write_part,
            )
        )
    )
    summed = lax.psum_scatter(partials, "kv", scatter_dimension=0, tiled=True)
    query_p, key_p, value_p, outgate_p, decay_p, write_p = tuple(
        (piece.astype(jnp.bfloat16).astype(jnp.float32) for piece in summed)
    )
    query = unit_rows(
        jax.nn.silu(query_p).reshape(seq_local, local_heads, key_size)
    ) * key_size ** (-0.5)
    keys = unit_rows(jax.nn.silu(key_p).reshape(seq_local, local_heads, key_size))
    vals = jax.nn.silu(value_p).reshape(seq_local, local_heads, value_size)
    outgate = outgate_p.reshape(seq_local, local_heads, value_size)
    beta = jax.nn.sigmoid(write_p)
    decay = -jnp.exp(decay_rate)[None, :] * jax.nn.softplus(decay_p)
    kept = state * jnp.exp(decay)[..., None, None]
    seen = jnp.einsum("bhk,bhkv->bhv", keys, kept, precision=lax.Precision.HIGHEST)
    delta = beta[..., None] * (vals - seen)
    new_state = kept + keys[..., :, None] * delta[..., None, :]
    outs = jnp.einsum("bhk,bhkv->bhv", query, new_state, precision=lax.Precision.HIGHEST)
    normed = outs * lax.rsqrt(jnp.mean(outs * outs, -1, keepdims=True) + rms_eps) * norm_gain
    heads_out = (
        (normed * jax.nn.silu(outgate))
        .astype(jnp.bfloat16)
        .reshape(seq_local, local_heads * value_size)
    )
    out_terms = jnp.dot(
        lax.all_gather(heads_out, "kv", axis=0, tiled=True),
        out_weight,
        preferred_element_type=jnp.float32,
    )
    mix = lax.psum_scatter(out_terms.astype(jnp.bfloat16), "tp", scatter_dimension=1, tiled=True)
    second = (residual_scale * mixed_own.astype(jnp.float32) + mix.astype(jnp.float32)).astype(
        jnp.bfloat16
    )
    second = lax.optimization_barrier(second)
    second_rows = lax.all_gather(second, ("kv", "tp"), axis=1, tiled=True)
    mlp_rows = whole_norm(second_rows, layer_gain[1])
    mlp_own = lax.dynamic_slice_in_dim(mlp_rows, own_start, own, 1)
    gate_two = jnp.dot(mlp_rows, gate_second, preferred_element_type=jnp.float32)
    up_two = jnp.dot(mlp_rows, up_second, preferred_element_type=jnp.float32)
    hidden_two = (jax.nn.silu(gate_two) * up_two).astype(jnp.bfloat16)
    terms_two = jnp.dot(hidden_two, down_second, preferred_element_type=jnp.float32)
    branch_two = lax.psum_scatter(terms_two, ("kv", "tp"), scatter_dimension=1, tiled=True)
    third = (residual_scale * mlp_own.astype(jnp.float32) + 0.5 * branch_two).astype(jnp.bfloat16)
    third = lax.optimization_barrier(third)
    gain_two = lax.dynamic_slice_in_dim(layer_gain[2], own_start, own)
    layer_out = spread_norm(third, gain_two, width)
    return (layer_out, new_state)


def dot(a, b):
    return jnp.dot(a, b, preferred_element_type=f32)


def dot_t(a, b):
    return lax.dot_general(a, b, (((1,), (1,)), ((), ())), preferred_element_type=f32)


def silu(x):
    return x * jax.nn.sigmoid(x)


def kernel(
    n_kv,
    n_tp,
    tokens,
    gate_first,
    up_first,
    down_first,
    gate_second,
    up_second,
    down_second,
    query_weight,
    key_weight,
    value_weight,
    outgate_weight,
    decay_weight,
    write_weight,
    decay_rate,
    norm_gain,
    layer_gain,
    out_weight,
    state,
    layer_out,
    new_state,
    tok,
    g1,
    u1,
    d1,
    g2,
    u2,
    d2,
    wq,
    wk,
    wv,
    wo,
    wd,
    ww,
    rate,
    ngain,
    lgain,
    ow,
    st,
    ns,
    out_v,
    red_out,
    red_in,
    red_out2,
    red_in2,
    gain_buf,
    pair_buf,
    stat_buf,
    proj_out,
    proj_in,
    head_buf,
    mix_out,
    mix_in,
    rows_buf,
    stat2_buf,
    stat_rows,
    load_sem,
    send_sem,
    recv_sem,
):
    n = n_kv * n_tp
    kv = lax.axis_index("kv")
    tp = lax.axis_index("tp")
    me = kv * n_tp + tp
    group, own = tokens.shape
    width = n * own
    block = wq.shape[0]
    seqs, heads, dk, dv = state.shape
    pairs = seqs * heads
    cols = heads * dk
    own_start = pl.multiple_of(me * own, own)
    block_start = pl.multiple_of(kv * block, block)

    loads = {}

    def load(name, src, dst):
        loads[name] = pltpu.make_async_copy(src, dst, load_sem.at[len(loads)])
        loads[name].start()

    load("tok", tokens, tok.at[me])
    load("g1", gate_first, g1)
    load("u1", up_first, u1)
    load("d1", down_first, d1)
    load("lgain", layer_gain, lgain)
    load("wq", query_weight, wq)
    load("wk", key_weight, wk)
    load("wv", value_weight, wv)
    load("wo", outgate_weight, wo)
    load("wd", decay_weight.at[:, pl.ds(block_start, block)], wd)
    load("ww", write_weight.at[:, pl.ds(block_start, block)], ww)
    load("rate", decay_rate, rate)
    load("ngain", norm_gain, ngain)
    load("st", state, st)
    load("ow", out_weight, ow)
    load("g2", gate_second, g2)
    load("u2", up_second, u2)
    load("d2", down_second, d2)

    def peer_of(step):
        other = lax.rem(me + step, n)
        return other, lax.div(other, n_tp), lax.rem(other, n_tp)

    barrier = pltpu.get_barrier_semaphore()
    for step in range(1, n):
        _, pk, pt = peer_of(step)
        pl.semaphore_signal(
            barrier,
            inc=1,
            device_id={"kv": pk, "tp": pt},
            device_id_type=pl.DeviceIdType.MESH,
        )
    pl.semaphore_wait(barrier, n - 1)

    sends = []

    def send(kind, src, dst, pk, pt):
        other = pk * n_tp + pt
        copy = pltpu.make_async_remote_copy(
            src_ref=src,
            dst_ref=dst,
            send_sem=send_sem.at[kind, other],
            recv_sem=recv_sem.at[kind, me],
            device_id={"kv": pk, "tp": pt},
            device_id_type=pl.DeviceIdType.MESH,
        )
        copy.start()
        sends.append(copy)

    def receive(kind, dst, pk, pt):
        other = pk * n_tp + pt
        pltpu.make_async_remote_copy(
            src_ref=dst,
            dst_ref=dst,
            send_sem=send_sem.at[kind, other],
            recv_sem=recv_sem.at[kind, other],
            device_id={"kv": pk, "tp": pt},
            device_id_type=pl.DeviceIdType.MESH,
        ).wait_recv()

    def send_all(kind, src_of, dst):
        for step in range(1, n):
            other, pk, pt = peer_of(step)
            send(kind, src_of(other), dst, pk, pt)

    def receive_all(kind, buf):
        for step in range(1, n):
            other, pk, pt = peer_of(step)
            receive(kind, buf.at[other], pk, pt)

    def send_kv(kind, src_of, dst):
        for step in range(1, n_kv):
            pk = lax.rem(kv + step, n_kv)
            send(kind, src_of(pk), dst, pk, tp)

    def receive_kv(kind, buf):
        for step in range(1, n_kv):
            pk = lax.rem(kv + step, n_kv)
            receive(kind, buf.at[pk], pk, tp)

    other_tp = lax.rem(tp + 1, n_tp)

    loads["tok"].wait()
    send_all(TOK, lambda other: tok.at[me], tok.at[me])
    loads["g1"].wait()
    loads["u1"].wait()
    receive_all(TOK, tok)

    def feed_forward(rows, gw, uw, dw, wait_down, send_buf):
        x = jnp.concatenate(rows, axis=1)
        hidden = (silu(dot_t(x, gw[...])) * dot_t(x, uw[...])).astype(bf16)
        wait_down()
        terms = dot(hidden, dw[...]).astype(bf16)
        for part in range(n):
            send_buf[part] = terms[:, part * own : (part + 1) * own]

    feed_forward([tok[s] for s in range(n)], g1, u1, d1, loads["d1"].wait, red_out)
    send_all(RED1, lambda other: red_out.at[other], red_in.at[me])
    red_in[me] = red_out[me]

    for name in ("lgain", "wq", "wk", "wv", "wo", "wd", "ww"):
        loads[name].wait()
    gain_block = lgain[0:1, pl.ds(block_start, block)]

    def project(x):
        parts = [dot(x, w[...]) for w in (wq, wk, wv, wo)]
        for w in (wd, ww):
            parts.append(dot_t(x, w[...]))
        return parts

    n_small = wd.shape[0]
    spans = [i * cols for i in range(4)] + [4 * cols, 4 * cols + 128]
    lengths = [cols] * 4 + [n_small] * 2
    gains = project(jnp.broadcast_to(gain_block, (group, block)).astype(bf16))
    gain_buf[kv] = jnp.zeros(gain_buf.shape[1:], f32)
    for part, start, length in zip(gains, spans, lengths):
        gain_buf[kv, :, start : start + length] = part[0:1]
    send_kv(GAINS, lambda pk: gain_buf.at[kv], gain_buf.at[kv])

    receive_all(RED1, red_in)
    branch = red_in[0].astype(f32)
    for s in range(1, n):
        branch = branch + red_in[s].astype(f32)
    first = (residual_scale * tok[me].astype(f32) + 0.5 * branch).astype(bf16)
    pair_buf[tp] = first
    send(PAIR, pair_buf.at[tp], pair_buf.at[tp], kv, other_tp)
    first = first.astype(f32)

    def sums(values):
        lane = lax.broadcasted_iota(jnp.int32, (group, 128), 1)
        total = jnp.sum(values, -1, keepdims=True)
        squares = jnp.sum(values * values, -1, keepdims=True)
        return jnp.where(lane == 0, total, jnp.where(lane == 1, squares, 0.0))

    stat_buf[me] = sums(first)
    send_all(STAT, lambda other: stat_buf.at[me], stat_buf.at[me])
    receive(PAIR, pair_buf.at[other_tp], kv, other_tp)
    rows = jnp.concatenate([pair_buf[t].astype(f32) for t in range(n_tp)], axis=1)
    centre = jnp.sum(rows, -1, keepdims=True) / block
    partial = project(((rows - centre) * gain_block).astype(bf16))
    for j in range(n_kv):
        proj_out[j] = jnp.zeros(proj_out.shape[1:], bf16)
        for part, start, length in zip(partial, spans, lengths):
            proj_out[j, :, start : start + length] = part[
                j * seqs : (j + 1) * seqs
            ].astype(bf16)
    send_kv(PROJ, lambda pk: proj_out.at[pk], proj_in.at[kv])
    proj_in[kv] = proj_out[kv]

    receive_all(STAT, stat_buf)
    receive_kv(GAINS, gain_buf)

    def moments(buf):
        total = buf[0]
        for s in range(1, n):
            total = total + buf[s]
        mean = total[:, 0:1] / width
        spread = total[:, 1:2] / width - mean * mean
        return mean, lax.rsqrt(spread + ln_eps)

    mean, rstd = moments(stat_buf)
    own_gain = lgain[0:1, pl.ds(own_start, own)]
    mixed_own = ((first - mean) * rstd * own_gain).astype(bf16).astype(f32)
    lane = lax.broadcasted_iota(jnp.int32, (group, 128), 1)
    packed = jnp.where(lane == n_kv, rstd, 0.0)
    for j in range(n_kv):
        local = stat_buf[j * n_tp]
        for t in range(1, n_tp):
            local = local + stat_buf[j * n_tp + t]
        packed = jnp.where(lane == j, local[:, 0:1] / block - mean, packed)
    stat_rows[...] = packed
    mine = stat_rows[pl.ds(kv * seqs, seqs), :]

    receive_kv(PROJ, proj_in)
    summed = jnp.zeros((seqs, proj_in.shape[2]), f32)
    for j in range(n_kv):
        summed = summed + proj_in[j].astype(f32) + mine[:, j : j + 1] * gain_buf[j]
    summed = (summed * mine[:, n_kv : n_kv + 1]).astype(bf16).astype(f32)

    def by_head(base):
        return jnp.concatenate(
            [
                summed[s : s + 1, base + h * dk : base + (h + 1) * dk]
                for s in range(seqs)
                for h in range(heads)
            ],
            axis=0,
        )

    def unit(values):
        return values * lax.rsqrt(jnp.sum(values * values, -1, keepdims=True) + rms_eps)

    query = unit(silu(by_head(0))) * dk ** (-0.5)
    keys = unit(silu(by_head(cols)))
    vals = silu(by_head(2 * cols))
    outgate = by_head(3 * cols)
    pair_lane = lax.broadcasted_iota(jnp.int32, (pairs, 128), 1)
    pair_head = lax.rem(lax.broadcasted_iota(jnp.int32, (pairs, 128), 0), heads)

    def per_head(base):
        spread = jnp.concatenate(
            [
                jnp.broadcast_to(summed[s : s + 1, base : base + 128], (heads, 128))
                for s in range(seqs)
            ],
            axis=0,
        )
        picked = jnp.where(pair_lane == pair_head + tp * heads, spread, 0.0)
        return jnp.sum(picked, -1, keepdims=True)

    decay_pre = per_head(4 * cols)
    beta = jax.nn.sigmoid(per_head(4 * cols + 128))
    loads["rate"].wait()
    rate_lane = lax.broadcasted_iota(jnp.int32, (pairs, heads), 1)
    rate_head = lax.rem(lax.broadcasted_iota(jnp.int32, (pairs, heads), 0), heads)
    rates = jnp.sum(
        jnp.where(rate_lane == rate_head, jnp.broadcast_to(rate[...], (pairs, heads)), 0.0),
        -1,
        keepdims=True,
    )
    softplus = jnp.maximum(decay_pre, 0.0) + jnp.log1p(jnp.exp(-jnp.abs(decay_pre)))
    factor = jnp.broadcast_to(jnp.exp(-jnp.exp(rates) * softplus), (pairs, dv))
    beta = jnp.broadcast_to(beta, (pairs, dv))
    keys_t = jnp.transpose(keys)
    query_t = jnp.transpose(query)
    loads["st"].wait()
    outs = []
    for s in range(seqs):
        for h in range(heads):
            i = s * heads + h
            kept = st[s, h] * factor[i : i + 1]
            key = keys_t[:, i : i + 1]
            seen = jnp.sum(kept * key, 0, keepdims=True)
            fresh = kept + key * (beta[i : i + 1] * (vals[i : i + 1] - seen))
            ns[s, h] = fresh
            outs.append(jnp.sum(fresh * query_t[:, i : i + 1], 0, keepdims=True))
    outs = jnp.concatenate(outs, axis=0)
    loads["ngain"].wait()
    normed = outs * lax.rsqrt(jnp.mean(outs * outs, -1, keepdims=True) + rms_eps) * ngain[...]
    gated = (normed * silu(outgate)).astype(bf16)
    for s in range(seqs):
        for h in range(heads):
            i = s * heads + h
            head_buf[kv, s : s + 1, h * dv : (h + 1) * dv] = gated[i : i + 1]
    send_kv(HEADS, lambda pk: head_buf.at[kv], head_buf.at[kv])
    store = pltpu.make_async_copy(ns, new_state, load_sem.at[len(loads)])
    store.start()
    loads["ow"].wait()
    receive_kv(HEADS, head_buf)
    everyone = jnp.concatenate([head_buf[j].astype(f32) for j in range(n_kv)], axis=0)
    terms = dot(everyone.astype(bf16), ow[...]).astype(bf16)
    for t in range(n_tp):
        mix_out[t] = terms[:, t * own : (t + 1) * own]
    send(MIX, mix_out.at[other_tp], mix_in, kv, other_tp)
    kept_half = mix_out[tp].astype(f32)
    receive(MIX, mix_in, kv, other_tp)
    mix = (kept_half + mix_in[...].astype(f32)).astype(bf16).astype(f32)
    rows_buf[me] = (residual_scale * mixed_own + mix).astype(bf16)
    send_all(ROWS2, lambda other: rows_buf.at[me], rows_buf.at[me])
    loads["g2"].wait()
    loads["u2"].wait()
    receive_all(ROWS2, rows_buf)

    second = [rows_buf[s].astype(f32) for s in range(n)]
    total = sum(jnp.sum(v, -1, keepdims=True) for v in second)
    squares = sum(jnp.sum(v * v, -1, keepdims=True) for v in second)
    mean = total / width
    rstd = lax.rsqrt(squares / width - mean * mean + ln_eps)

    def normalise(v, start):
        return ((v - mean) * rstd * lgain[1:2, pl.ds(start, own)]).astype(bf16)

    mlp_own = normalise(rows_buf[me].astype(f32), own_start).astype(f32)
    feed_forward(
        [normalise(v, s * own) for s, v in enumerate(second)],
        g2,
        u2,
        d2,
        loads["d2"].wait,
        red_out2,
    )
    send_all(RED2, lambda other: red_out2.at[other], red_in2.at[me])
    red_in2[me] = red_out2[me]
    receive_all(RED2, red_in2)
    branch = red_in2[0].astype(f32)
    for s in range(1, n):
        branch = branch + red_in2[s].astype(f32)
    third = (residual_scale * mlp_own + 0.5 * branch).astype(bf16).astype(f32)
    stat2_buf[me] = sums(third)
    send_all(STAT2, lambda other: stat2_buf.at[me], stat2_buf.at[me])
    receive_all(STAT2, stat2_buf)
    mean, rstd = moments(stat2_buf)
    out_v[...] = ((third - mean) * rstd * lgain[2:3, pl.ds(own_start, own)]).astype(bf16)
    final = pltpu.make_async_copy(out_v, layer_out, load_sem.at[len(loads) + 1])
    final.start()
    for copy in sends:
        copy.wait_send()
    store.wait()
    final.wait()


def shards(n_kv, n_tp, *args):
    if args[0].shape[1] % 128 or args[17].shape[2] != 128:
        return shards_by_collectives(*args)
    args = list(args)
    for i in (1, 2, 4, 5, 11, 12):
        args[i] = args[i].T
    args[13] = args[13].reshape(1, -1)
    args[14] = args[14].reshape(1, -1)
    tokens, decay_weight, state = args[0], args[11], args[17]
    query_weight = args[7]
    n = n_kv * n_tp
    group, own = tokens.shape
    seqs = state.shape[0]
    block, cols = query_weight.shape
    small = decay_weight.shape[0]
    flat = 4 * cols + 2 * 128

    def like(x):
        return pltpu.VMEM(x.shape, x.dtype)

    scratch = [
        pltpu.VMEM((n, group, own), bf16),
        *[like(x) for x in args[1:11]],
        pltpu.VMEM((small, block), bf16),
        pltpu.VMEM((small, block), bf16),
        *[like(x) for x in args[13:18]],
        like(state),
        like(tokens),
        pltpu.VMEM((n, group, own), bf16),
        pltpu.VMEM((n, group, own), bf16),
        pltpu.VMEM((n, group, own), bf16),
        pltpu.VMEM((n, group, own), bf16),
        pltpu.VMEM((n_kv, 1, flat), f32),
        pltpu.VMEM((n_tp, group, own), bf16),
        pltpu.VMEM((n, group, 128), f32),
        pltpu.VMEM((n_kv, seqs, flat), bf16),
        pltpu.VMEM((n_kv, seqs, flat), bf16),
        pltpu.VMEM((n_kv, seqs, cols), bf16),
        pltpu.VMEM((n_tp, group, own), bf16),
        pltpu.VMEM((group, own), bf16),
        pltpu.VMEM((n, group, own), bf16),
        pltpu.VMEM((n, group, 128), f32),
        pltpu.VMEM((group, 128), f32),
        pltpu.SemaphoreType.DMA((20,)),
        pltpu.SemaphoreType.DMA((11, n)),
        pltpu.SemaphoreType.DMA((11, n)),
    ]
    return pl.pallas_call(
        functools.partial(kernel, n_kv, n_tp),
        out_shape=(
            jax.ShapeDtypeStruct(tokens.shape, tokens.dtype),
            jax.ShapeDtypeStruct(state.shape, state.dtype),
        ),
        in_specs=[pl.BlockSpec(memory_space=pl.ANY)] * len(args),
        out_specs=(pl.BlockSpec(memory_space=pl.ANY),) * 2,
        scratch_shapes=scratch,
        compiler_params=pltpu.CompilerParams(
            collective_id=0, has_side_effects=True, vmem_limit_bytes=60 * 1024 * 1024
        ),
    )(*args)


def solution(mesh):
    in_specs = (
        P("dp", ("kv", "tp")),
        P(None, ("kv", "tp")),
        P(None, ("kv", "tp")),
        P(("kv", "tp"), None),
        P(None, ("kv", "tp")),
        P(None, ("kv", "tp")),
        P(("kv", "tp"), None),
        P("kv", "tp"),
        P("kv", "tp"),
        P("kv", "tp"),
        P("kv", "tp"),
        P(),
        P(),
        P("tp"),
        P(),
        P(),
        P("tp", "kv"),
        P(("dp", "kv"), "tp", None, None),
    )
    out_specs = (P("dp", ("kv", "tp")), P(("dp", "kv"), "tp", None, None))
    body = functools.partial(shards, mesh.shape["kv"], mesh.shape["tp"])
    return jax.shard_map(body, mesh=mesh, in_specs=in_specs, out_specs=out_specs, check_vma=False)
```

```python
import functools

import jax
import jax.numpy as jnp
from jax import lax
from jax.experimental import pallas as pl
from jax.experimental.pallas import tpu as pltpu
from jax.sharding import PartitionSpec as P

residual_scale = 2.0**0.25
ln_eps = 1e-05
rms_eps = 1e-06
f32 = jnp.float32
bf16 = jnp.bfloat16

TOK, RED1, GAINS, FIRST, PROJ, HEADS, MIX, RED2, STAT2 = range(9)


def finish_norm(values, total, squares, width, gain):
    mean = total[:, None] / width
    spread = squares[:, None] / width - mean * mean
    return ((values - mean) * lax.rsqrt(spread + ln_eps) * gain).astype(jnp.bfloat16)


def spread_norm(rows, gain, width):
    values = rows.astype(jnp.float32)
    total, squares = lax.psum((jnp.sum(values, -1), jnp.sum(values * values, -1)), ("kv", "tp"))
    return finish_norm(values, total, squares, width, gain)


def whole_norm(rows, gain):
    values = rows.astype(jnp.float32)
    return finish_norm(
        values, jnp.sum(values, -1), jnp.sum(values * values, -1), values.shape[1], gain
    )


def unit_rows(values):
    return values * lax.rsqrt(jnp.sum(values * values, -1, keepdims=True) + rms_eps)


def shards_by_collectives(
    tokens,
    gate_first,
    up_first,
    down_first,
    gate_second,
    up_second,
    down_second,
    query_weight,
    key_weight,
    value_weight,
    outgate_weight,
    decay_weight,
    write_weight,
    decay_rate,
    norm_gain,
    layer_gain,
    out_weight,
    state,
):
    kv_index = lax.axis_index("kv")
    tp_index = lax.axis_index("tp")
    width = decay_weight.shape[0]
    own = tokens.shape[1]
    block = query_weight.shape[0]
    local_heads = decay_rate.shape[0]
    key_size = state.shape[2]
    value_size = state.shape[3]
    seq_local = state.shape[0]
    own_start = (kv_index * lax.axis_size("tp") + tp_index) * own
    block_start = kv_index * block
    fold_piece = lax.all_gather(tokens, ("kv", "tp"), axis=1, tiled=True)
    gate = jnp.dot(fold_piece, gate_first, preferred_element_type=jnp.float32)
    up = jnp.dot(fold_piece, up_first, preferred_element_type=jnp.float32)
    hidden = (jax.nn.silu(gate) * up).astype(jnp.bfloat16)
    terms = jnp.dot(hidden, down_first, preferred_element_type=jnp.float32)
    branch = lax.psum_scatter(terms, ("kv", "tp"), scatter_dimension=1, tiled=True)
    first = (residual_scale * tokens.astype(jnp.float32) + 0.5 * branch).astype(jnp.bfloat16)
    first = lax.optimization_barrier(first)
    first_rows = lax.all_gather(first, ("kv", "tp"), axis=1, tiled=True)
    mixed_rows = whole_norm(first_rows, layer_gain[0])
    mixed_own = lax.dynamic_slice_in_dim(mixed_rows, own_start, own, 1)
    mixed_block = lax.dynamic_slice_in_dim(mixed_rows, block_start, block, 1)
    decay_part = lax.dynamic_slice(
        decay_weight, (block_start, tp_index * local_heads), (block, local_heads)
    )
    write_part = lax.dynamic_slice(
        write_weight, (block_start, tp_index * local_heads), (block, local_heads)
    )
    partials = tuple(
        (
            jnp.dot(mixed_block, weight, preferred_element_type=jnp.float32)
            for weight in (
                query_weight,
                key_weight,
                value_weight,
                outgate_weight,
                decay_part,
                write_part,
            )
        )
    )
    summed = lax.psum_scatter(partials, "kv", scatter_dimension=0, tiled=True)
    query_p, key_p, value_p, outgate_p, decay_p, write_p = tuple(
        (piece.astype(jnp.bfloat16).astype(jnp.float32) for piece in summed)
    )
    query = unit_rows(
        jax.nn.silu(query_p).reshape(seq_local, local_heads, key_size)
    ) * key_size ** (-0.5)
    keys = unit_rows(jax.nn.silu(key_p).reshape(seq_local, local_heads, key_size))
    vals = jax.nn.silu(value_p).reshape(seq_local, local_heads, value_size)
    outgate = outgate_p.reshape(seq_local, local_heads, value_size)
    beta = jax.nn.sigmoid(write_p)
    decay = -jnp.exp(decay_rate)[None, :] * jax.nn.softplus(decay_p)
    kept = state * jnp.exp(decay)[..., None, None]
    seen = jnp.einsum("bhk,bhkv->bhv", keys, kept, precision=lax.Precision.HIGHEST)
    delta = beta[..., None] * (vals - seen)
    new_state = kept + keys[..., :, None] * delta[..., None, :]
    outs = jnp.einsum("bhk,bhkv->bhv", query, new_state, precision=lax.Precision.HIGHEST)
    normed = outs * lax.rsqrt(jnp.mean(outs * outs, -1, keepdims=True) + rms_eps) * norm_gain
    heads_out = (
        (normed * jax.nn.silu(outgate))
        .astype(jnp.bfloat16)
        .reshape(seq_local, local_heads * value_size)
    )
    out_terms = jnp.dot(
        lax.all_gather(heads_out, "kv", axis=0, tiled=True),
        out_weight,
        preferred_element_type=jnp.float32,
    )
    mix = lax.psum_scatter(out_terms.astype(jnp.bfloat16), "tp", scatter_dimension=1, tiled=True)
    second = (residual_scale * mixed_own.astype(jnp.float32) + mix.astype(jnp.float32)).astype(
        jnp.bfloat16
    )
    second = lax.optimization_barrier(second)
    second_rows = lax.all_gather(second, ("kv", "tp"), axis=1, tiled=True)
    mlp_rows = whole_norm(second_rows, layer_gain[1])
    mlp_own = lax.dynamic_slice_in_dim(mlp_rows, own_start, own, 1)
    gate_two = jnp.dot(mlp_rows, gate_second, preferred_element_type=jnp.float32)
    up_two = jnp.dot(mlp_rows, up_second, preferred_element_type=jnp.float32)
    hidden_two = (jax.nn.silu(gate_two) * up_two).astype(jnp.bfloat16)
    terms_two = jnp.dot(hidden_two, down_second, preferred_element_type=jnp.float32)
    branch_two = lax.psum_scatter(terms_two, ("kv", "tp"), scatter_dimension=1, tiled=True)
    third = (residual_scale * mlp_own.astype(jnp.float32) + 0.5 * branch_two).astype(jnp.bfloat16)
    third = lax.optimization_barrier(third)
    gain_two = lax.dynamic_slice_in_dim(layer_gain[2], own_start, own)
    layer_out = spread_norm(third, gain_two, width)
    return (layer_out, new_state)


def dot(a, b):
    return jnp.dot(a, b, preferred_element_type=f32)


def dot_t(a, b):
    return lax.dot_general(a, b, (((1,), (1,)), ((), ())), preferred_element_type=f32)


def silu(x):
    return x * jax.nn.sigmoid(x)


def kernel(
    n_kv,
    n_tp,
    tokens,
    gate_first,
    up_first,
    down_first,
    gate_second,
    up_second,
    down_second,
    query_weight,
    key_weight,
    value_weight,
    outgate_weight,
    decay_weight,
    write_weight,
    decay_rate,
    norm_gain,
    layer_gain,
    out_weight,
    state,
    layer_out,
    new_state,
    tok,
    g1,
    u1,
    d1,
    g2,
    u2,
    d2,
    wq,
    wk,
    wv,
    wo,
    wd,
    ww,
    rate,
    ngain,
    lgain,
    ow,
    st,
    ns,
    out_v,
    red_out,
    red_in,
    red_out2,
    red_in2,
    gain_buf,
    first_buf,
    proj_out,
    proj_in,
    head_buf,
    mix_buf,
    mixed_buf,
    own_block,
    stat2_buf,
    stat_rows,
    load_sem,
    send_sem,
    recv_sem,
):
    n = n_kv * n_tp
    kv = lax.axis_index("kv")
    tp = lax.axis_index("tp")
    me = kv * n_tp + tp
    group, own = tokens.shape
    width = n * own
    block = wq.shape[0]
    seqs, heads, dk, dv = state.shape
    pairs = seqs * heads
    cols = heads * dk
    block_start = pl.multiple_of(kv * block, block)

    loads = {}

    def load(name, src, dst):
        loads[name] = pltpu.make_async_copy(src, dst, load_sem.at[len(loads)])
        loads[name].start()

    load("tok", tokens, tok.at[me])
    load("g1", gate_first, g1)
    load("u1", up_first, u1)
    load("d1", down_first, d1)
    load("lgain", layer_gain, lgain)
    load("wq", query_weight, wq)
    load("wk", key_weight, wk)
    load("wv", value_weight, wv)
    load("wo", outgate_weight, wo)
    load("wd", decay_weight.at[:, pl.ds(block_start, block)], wd)
    load("ww", write_weight.at[:, pl.ds(block_start, block)], ww)
    load("rate", decay_rate, rate)
    load("ngain", norm_gain, ngain)
    load("st", state, st)
    load("ow", out_weight, ow)
    load("g2", gate_second, g2)
    load("u2", up_second, u2)
    load("d2", down_second, d2)

    ring = sorted(range(n_kv), key=lambda d: min(d, n_kv - d))
    near = [(dk, dt) for dk in ring for dt in range(n_tp)]
    partners = [p for p in near if p[0] == 0 and p[1]]
    far = [p for p in near if p[0]][::-1]

    def peer_of(step):
        pk = lax.rem(kv + step[0], n_kv)
        pt = lax.rem(tp + step[1], n_tp)
        return pk * n_tp + pt, pk, pt

    barrier = pltpu.get_barrier_semaphore()
    for step in far + partners:
        _, pk, pt = peer_of(step)
        pl.semaphore_signal(
            barrier,
            inc=1,
            device_id={"kv": pk, "tp": pt},
            device_id_type=pl.DeviceIdType.MESH,
        )
    pl.semaphore_wait(barrier, n - 1)

    sends = []

    def send(kind, src, dst, pk, pt):
        other = pk * n_tp + pt
        copy = pltpu.make_async_remote_copy(
            src_ref=src,
            dst_ref=dst,
            send_sem=send_sem.at[kind, other],
            recv_sem=recv_sem.at[kind, me],
            device_id={"kv": pk, "tp": pt},
            device_id_type=pl.DeviceIdType.MESH,
        )
        copy.start()
        sends.append(copy)

    def receive(kind, dst, pk, pt):
        other = pk * n_tp + pt
        pltpu.make_async_remote_copy(
            src_ref=dst,
            dst_ref=dst,
            send_sem=send_sem.at[kind, other],
            recv_sem=recv_sem.at[kind, other],
            device_id={"kv": pk, "tp": pt},
            device_id_type=pl.DeviceIdType.MESH,
        ).wait_recv()

    def send_all(kind, src_of, dst):
        for step in partners + far:
            other, pk, pt = peer_of(step)
            send(kind, src_of(other), dst, pk, pt)

    def receive_all(kind, buf):
        for step in near[1:]:
            other, pk, pt = peer_of(step)
            receive(kind, buf.at[other], pk, pt)

    def send_kv(kind, src_of, dst):
        for step in ring[:0:-1]:
            pk = lax.rem(kv + step, n_kv)
            send(kind, src_of(pk), dst, pk, tp)

    def receive_kv(kind, buf):
        for step in range(1, n_kv):
            pk = lax.rem(kv + step, n_kv)
            receive(kind, buf.at[pk], pk, tp)

    other_tp = lax.rem(tp + 1, n_tp)

    loads["tok"].wait()
    send_all(TOK, lambda other: tok.at[me], tok.at[me])
    loads["g1"].wait()
    loads["u1"].wait()

    def slot(other):
        return pl.ds(pl.multiple_of(other * own, own), own)

    def send_shares(kind, hidden, dw, send_buf, recv_buf):
        for step in far + partners:
            other, pk, pt = peer_of(step)
            send_buf[other] = dot(hidden, dw[:, slot(other)]).astype(bf16)
            send(kind, send_buf.at[other], recv_buf.at[me], pk, pt)
        recv_buf[me] = dot(hidden, dw[:, slot(me)]).astype(bf16)

    gate, up = 0.0, 0.0
    for step in near:
        other, pk, pt = peer_of(step)
        if step != (0, 0):
            receive(TOK, tok.at[other], pk, pt)
        gate = gate + dot_t(tok[other], g1[:, slot(other)])
        up = up + dot_t(tok[other], u1[:, slot(other)])
    hidden = (silu(gate) * up).astype(bf16)
    loads["d1"].wait()
    send_shares(RED1, hidden, d1, red_out, red_in)

    for name in ("lgain", "wq", "wk", "wv", "wo", "wd", "ww"):
        loads[name].wait()
    gain_block = lgain[0:1, pl.ds(block_start, block)]

    def project(x):
        parts = [dot(x, w[...]) for w in (wq, wk, wv, wo)]
        for w in (wd, ww):
            parts.append(dot_t(x, w[...]))
        return parts

    n_small = wd.shape[0]
    spans = [i * cols for i in range(4)] + [4 * cols, 4 * cols + 128]
    lengths = [cols] * 4 + [n_small] * 2
    gains = project(jnp.broadcast_to(gain_block, (group, block)).astype(bf16))
    gain_buf[kv] = jnp.zeros(gain_buf.shape[1:], f32)
    for part, start, length in zip(gains, spans, lengths):
        gain_buf[kv, :, start : start + length] = part[0:1]
    send_kv(GAINS, lambda pk: gain_buf.at[kv], gain_buf.at[kv])

    receive_all(RED1, red_in)
    branch = red_in[0].astype(f32)
    for s in range(1, n):
        branch = branch + red_in[s].astype(f32)
    first = (residual_scale * tok[me].astype(f32) + 0.5 * branch).astype(bf16)
    first_buf[me] = first
    send_all(FIRST, lambda other: first_buf.at[me], first_buf.at[me])
    for step in partners:
        other, pk, pt = peer_of(step)
        receive(FIRST, first_buf.at[other], pk, pt)
    rows = jnp.concatenate(
        [first_buf[kv * n_tp + t].astype(f32) for t in range(n_tp)], axis=1
    )
    centre = jnp.sum(rows, -1, keepdims=True) / block
    partial = project(((rows - centre) * gain_block).astype(bf16))
    for j in range(n_kv):
        proj_out[j] = jnp.zeros(proj_out.shape[1:], bf16)
        for part, start, length in zip(partial, spans, lengths):
            proj_out[j, :, start : start + length] = part[
                j * seqs : (j + 1) * seqs
            ].astype(bf16)
    send_kv(PROJ, lambda pk: proj_out.at[pk], proj_in.at[kv])
    proj_in[kv] = proj_out[kv]

    for step in near[n_tp:]:
        other, pk, pt = peer_of(step)
        receive(FIRST, first_buf.at[other], pk, pt)
    receive_kv(GAINS, gain_buf)

    def sums(values):
        total = jnp.sum(values, -1, keepdims=True)
        squares = jnp.sum(values * values, -1, keepdims=True)
        return jnp.where(lane == 0, total, jnp.where(lane == 1, squares, 0.0))

    def moments(total, squares):
        mean = total / width
        return mean, lax.rsqrt(squares / width - mean * mean + ln_eps)

    values = [first_buf[s].astype(f32) for s in range(n)]
    totals = [jnp.sum(v, -1, keepdims=True) for v in values]
    squares = sum(jnp.sum(v * v, -1, keepdims=True) for v in values)
    mean, rstd = moments(sum(totals), squares)
    lane = lax.broadcasted_iota(jnp.int32, (group, 128), 1)
    packed = jnp.where(lane == n_kv, rstd, 0.0)
    for j in range(n_kv):
        local = sum(totals[j * n_tp : (j + 1) * n_tp])
        packed = jnp.where(lane == j, local / block - mean, packed)
    stat_rows[...] = packed
    mine = stat_rows[pl.ds(kv * seqs, seqs), :]

    receive_kv(PROJ, proj_in)
    summed = jnp.zeros((seqs, proj_in.shape[2]), f32)
    for j in range(n_kv):
        summed = summed + proj_in[j].astype(f32) + mine[:, j : j + 1] * gain_buf[j]
    summed = (summed * mine[:, n_kv : n_kv + 1]).astype(bf16).astype(f32)

    def by_head(base):
        return jnp.concatenate(
            [
                summed[s : s + 1, base + h * dk : base + (h + 1) * dk]
                for s in range(seqs)
                for h in range(heads)
            ],
            axis=0,
        )

    def unit(values):
        return values * lax.rsqrt(jnp.sum(values * values, -1, keepdims=True) + rms_eps)

    query = unit(silu(by_head(0))) * dk ** (-0.5)
    keys = unit(silu(by_head(cols)))
    vals = silu(by_head(2 * cols))
    outgate = by_head(3 * cols)
    pair_lane = lax.broadcasted_iota(jnp.int32, (pairs, 128), 1)
    pair_head = lax.rem(lax.broadcasted_iota(jnp.int32, (pairs, 128), 0), heads)

    def per_head(base):
        spread = jnp.concatenate(
            [
                jnp.broadcast_to(summed[s : s + 1, base : base + 128], (heads, 128))
                for s in range(seqs)
            ],
            axis=0,
        )
        picked = jnp.where(pair_lane == pair_head + tp * heads, spread, 0.0)
        return jnp.sum(picked, -1, keepdims=True)

    decay_pre = per_head(4 * cols)
    beta = jax.nn.sigmoid(per_head(4 * cols + 128))
    loads["rate"].wait()
    rate_lane = lax.broadcasted_iota(jnp.int32, (pairs, heads), 1)
    rate_head = lax.rem(lax.broadcasted_iota(jnp.int32, (pairs, heads), 0), heads)
    rates = jnp.sum(
        jnp.where(rate_lane == rate_head, jnp.broadcast_to(rate[...], (pairs, heads)), 0.0),
        -1,
        keepdims=True,
    )
    softplus = jnp.maximum(decay_pre, 0.0) + jnp.log1p(jnp.exp(-jnp.abs(decay_pre)))
    factor = jnp.broadcast_to(jnp.exp(-jnp.exp(rates) * softplus), (pairs, dv))
    beta = jnp.broadcast_to(beta, (pairs, dv))
    keys_t = jnp.transpose(keys)
    query_t = jnp.transpose(query)
    loads["st"].wait()
    outs = []
    for s in range(seqs):
        for h in range(heads):
            i = s * heads + h
            kept = st[s, h] * factor[i : i + 1]
            key = keys_t[:, i : i + 1]
            seen = jnp.sum(kept * key, 0, keepdims=True)
            fresh = kept + key * (beta[i : i + 1] * (vals[i : i + 1] - seen))
            ns[s, h] = fresh
            outs.append(jnp.sum(fresh * query_t[:, i : i + 1], 0, keepdims=True))
    outs = jnp.concatenate(outs, axis=0)
    loads["ngain"].wait()
    normed = outs * lax.rsqrt(jnp.mean(outs * outs, -1, keepdims=True) + rms_eps) * ngain[...]
    gated = (normed * silu(outgate)).astype(bf16)
    for s in range(seqs):
        for h in range(heads):
            i = s * heads + h
            head_buf[kv, s : s + 1, h * dv : (h + 1) * dv] = gated[i : i + 1]
    send_kv(HEADS, lambda pk: head_buf.at[kv], head_buf.at[kv])
    store = pltpu.make_async_copy(ns, new_state, load_sem.at[len(loads)])
    store.start()
    for s in range(n):
        scaled = (values[s] - mean) * rstd * lgain[0:1, s * own : (s + 1) * own]
        mixed_buf[s] = scaled.astype(bf16)
    loads["ow"].wait()
    receive_kv(HEADS, head_buf)
    everyone = jnp.concatenate([head_buf[j].astype(f32) for j in range(n_kv)], axis=0)
    mix_buf[me] = dot(everyone.astype(bf16), ow[...]).astype(bf16)
    send_all(MIX, lambda other: mix_buf.at[me], mix_buf.at[me])
    loads["g2"].wait()
    loads["u2"].wait()

    gate, up, total, squares = 0.0, 0.0, 0.0, 0.0
    centre = None
    for hop in ring:
        for dt in range(n_tp):
            other, pk, pt = peer_of((hop, dt))
            if (hop, dt) != (0, 0):
                receive(MIX, mix_buf.at[other], pk, pt)
        pk = lax.rem(kv + hop, n_kv)
        mix = mix_buf[pk * n_tp].astype(f32)
        for t in range(1, n_tp):
            mix = mix + mix_buf[pk * n_tp + t].astype(f32)
        mixed = jnp.concatenate([mixed_buf[pk * n_tp + t] for t in range(n_tp)], axis=1)
        second = residual_scale * mixed.astype(f32) + mix.astype(bf16).astype(f32)
        second = second.astype(bf16).astype(f32)
        sub = jnp.sum(second, -1, keepdims=True)
        if centre is None:
            centre = sub / block
            own_block[...] = second
        total = total + sub
        squares = squares + jnp.sum(second * second, -1, keepdims=True)
        span = pl.ds(pl.multiple_of(pk * block, block), block)
        gain = lgain[1:2, span]
        x = jnp.concatenate(
            [(second - centre) * gain, jnp.broadcast_to(gain, (group, block))], axis=0
        ).astype(bf16)
        gate = gate + dot_t(x, g2[:, span])
        up = up + dot_t(x, u2[:, span])
    mean, rstd = moments(total, squares)
    shift = mean - centre
    gate = rstd * (gate[:group] - shift * gate[group : group + 1])
    up = rstd * (up[:group] - shift * up[group : group + 1])
    hidden = (silu(gate) * up).astype(bf16)
    loads["d2"].wait()
    send_shares(RED2, hidden, d2, red_out2, red_in2)
    second_own = own_block[:, slot(tp)]
    mlp_own = (second_own - mean) * rstd * lgain[1:2, slot(me)]
    mlp_own = mlp_own.astype(bf16).astype(f32)
    receive_all(RED2, red_in2)
    branch = red_in2[0].astype(f32)
    for s in range(1, n):
        branch = branch + red_in2[s].astype(f32)
    third = (residual_scale * mlp_own + 0.5 * branch).astype(bf16).astype(f32)
    stat2_buf[me] = sums(third)
    send_all(STAT2, lambda other: stat2_buf.at[me], stat2_buf.at[me])
    receive_all(STAT2, stat2_buf)
    total = stat2_buf[0]
    for s in range(1, n):
        total = total + stat2_buf[s]
    mean, rstd = moments(total[:, 0:1], total[:, 1:2])
    out_v[...] = ((third - mean) * rstd * lgain[2:3, slot(me)]).astype(bf16)
    final = pltpu.make_async_copy(out_v, layer_out, load_sem.at[len(loads) + 1])
    final.start()
    for copy in sends:
        copy.wait_send()
    store.wait()
    final.wait()


def shards(n_kv, n_tp, *args):
    if args[0].shape[1] % 128 or args[17].shape[2] != 128:
        return shards_by_collectives(*args)
    args = list(args)
    for i in (1, 2, 4, 5, 11, 12):
        args[i] = args[i].T
    args[13] = args[13].reshape(1, -1)
    args[14] = args[14].reshape(1, -1)
    tokens, decay_weight, state = args[0], args[11], args[17]
    query_weight = args[7]
    n = n_kv * n_tp
    group, own = tokens.shape
    seqs = state.shape[0]
    block, cols = query_weight.shape
    small = decay_weight.shape[0]
    flat = 4 * cols + 2 * 128

    def like(x):
        return pltpu.VMEM(x.shape, x.dtype)

    scratch = [
        pltpu.VMEM((n, group, own), bf16),
        *[like(x) for x in args[1:11]],
        pltpu.VMEM((small, block), bf16),
        pltpu.VMEM((small, block), bf16),
        *[like(x) for x in args[13:18]],
        like(state),
        like(tokens),
        pltpu.VMEM((n, group, own), bf16),
        pltpu.VMEM((n, group, own), bf16),
        pltpu.VMEM((n, group, own), bf16),
        pltpu.VMEM((n, group, own), bf16),
        pltpu.VMEM((n_kv, 1, flat), f32),
        pltpu.VMEM((n, group, own), bf16),
        pltpu.VMEM((n_kv, seqs, flat), bf16),
        pltpu.VMEM((n_kv, seqs, flat), bf16),
        pltpu.VMEM((n_kv, seqs, cols), bf16),
        pltpu.VMEM((n, group, n_tp * own), bf16),
        pltpu.VMEM((n, group, own), bf16),
        pltpu.VMEM((group, n_tp * own), f32),
        pltpu.VMEM((n, group, 128), f32),
        pltpu.VMEM((group, 128), f32),
        pltpu.SemaphoreType.DMA((20,)),
        pltpu.SemaphoreType.DMA((9, n)),
        pltpu.SemaphoreType.DMA((9, n)),
    ]
    return pl.pallas_call(
        functools.partial(kernel, n_kv, n_tp),
        out_shape=(
            jax.ShapeDtypeStruct(tokens.shape, tokens.dtype),
            jax.ShapeDtypeStruct(state.shape, state.dtype),
        ),
        in_specs=[pl.BlockSpec(memory_space=pl.ANY)] * len(args),
        out_specs=(pl.BlockSpec(memory_space=pl.ANY),) * 2,
        scratch_shapes=scratch,
        compiler_params=pltpu.CompilerParams(
            collective_id=0, has_side_effects=True, vmem_limit_bytes=60 * 1024 * 1024
        ),
    )(*args)


def solution(mesh):
    in_specs = (
        P("dp", ("kv", "tp")),
        P(None, ("kv", "tp")),
        P(None, ("kv", "tp")),
        P(("kv", "tp"), None),
        P(None, ("kv", "tp")),
        P(None, ("kv", "tp")),
        P(("kv", "tp"), None),
        P("kv", "tp"),
        P("kv", "tp"),
        P("kv", "tp"),
        P("kv", "tp"),
        P(),
        P(),
        P("tp"),
        P(),
        P(),
        P("tp", "kv"),
        P(("dp", "kv"), "tp", None, None),
    )
    out_specs = (P("dp", ("kv", "tp")), P(("dp", "kv"), "tp", None, None))
    body = functools.partial(shards, mesh.shape["kv"], mesh.shape["tp"])
    return jax.shard_map(body, mesh=mesh, in_specs=in_specs, out_specs=out_specs, check_vma=False)
```

```python
import functools

import jax
import jax.numpy as jnp
from jax import lax
from jax.experimental import pallas as pl
from jax.experimental.pallas import tpu as pltpu
from jax.sharding import PartitionSpec as P

residual_scale = 2.0**0.25
ln_eps = 1e-05
rms_eps = 1e-06
f32 = jnp.float32
bf16 = jnp.bfloat16

TOK, RED1, GAINS, FIRST, PROJ, HEADS, MIX, RED2, STAT2 = range(9)


def finish_norm(values, total, squares, width, gain):
    mean = total[:, None] / width
    spread = squares[:, None] / width - mean * mean
    return ((values - mean) * lax.rsqrt(spread + ln_eps) * gain).astype(jnp.bfloat16)


def spread_norm(rows, gain, width):
    values = rows.astype(jnp.float32)
    total, squares = lax.psum((jnp.sum(values, -1), jnp.sum(values * values, -1)), ("kv", "tp"))
    return finish_norm(values, total, squares, width, gain)


def whole_norm(rows, gain):
    values = rows.astype(jnp.float32)
    return finish_norm(
        values, jnp.sum(values, -1), jnp.sum(values * values, -1), values.shape[1], gain
    )


def unit_rows(values):
    return values * lax.rsqrt(jnp.sum(values * values, -1, keepdims=True) + rms_eps)


def shards_by_collectives(
    tokens,
    gate_first,
    up_first,
    down_first,
    gate_second,
    up_second,
    down_second,
    query_weight,
    key_weight,
    value_weight,
    outgate_weight,
    decay_weight,
    write_weight,
    decay_rate,
    norm_gain,
    layer_gain,
    out_weight,
    state,
):
    kv_index = lax.axis_index("kv")
    tp_index = lax.axis_index("tp")
    width = decay_weight.shape[0]
    own = tokens.shape[1]
    block = query_weight.shape[0]
    local_heads = decay_rate.shape[0]
    key_size = state.shape[2]
    value_size = state.shape[3]
    seq_local = state.shape[0]
    own_start = (kv_index * lax.axis_size("tp") + tp_index) * own
    block_start = kv_index * block
    fold_piece = lax.all_gather(tokens, ("kv", "tp"), axis=1, tiled=True)
    gate = jnp.dot(fold_piece, gate_first, preferred_element_type=jnp.float32)
    up = jnp.dot(fold_piece, up_first, preferred_element_type=jnp.float32)
    hidden = (jax.nn.silu(gate) * up).astype(jnp.bfloat16)
    terms = jnp.dot(hidden, down_first, preferred_element_type=jnp.float32)
    branch = lax.psum_scatter(terms, ("kv", "tp"), scatter_dimension=1, tiled=True)
    first = (residual_scale * tokens.astype(jnp.float32) + 0.5 * branch).astype(jnp.bfloat16)
    first = lax.optimization_barrier(first)
    first_rows = lax.all_gather(first, ("kv", "tp"), axis=1, tiled=True)
    mixed_rows = whole_norm(first_rows, layer_gain[0])
    mixed_own = lax.dynamic_slice_in_dim(mixed_rows, own_start, own, 1)
    mixed_block = lax.dynamic_slice_in_dim(mixed_rows, block_start, block, 1)
    decay_part = lax.dynamic_slice(
        decay_weight, (block_start, tp_index * local_heads), (block, local_heads)
    )
    write_part = lax.dynamic_slice(
        write_weight, (block_start, tp_index * local_heads), (block, local_heads)
    )
    partials = tuple(
        (
            jnp.dot(mixed_block, weight, preferred_element_type=jnp.float32)
            for weight in (
                query_weight,
                key_weight,
                value_weight,
                outgate_weight,
                decay_part,
                write_part,
            )
        )
    )
    summed = lax.psum_scatter(partials, "kv", scatter_dimension=0, tiled=True)
    query_p, key_p, value_p, outgate_p, decay_p, write_p = tuple(
        (piece.astype(jnp.bfloat16).astype(jnp.float32) for piece in summed)
    )
    query = unit_rows(
        jax.nn.silu(query_p).reshape(seq_local, local_heads, key_size)
    ) * key_size ** (-0.5)
    keys = unit_rows(jax.nn.silu(key_p).reshape(seq_local, local_heads, key_size))
    vals = jax.nn.silu(value_p).reshape(seq_local, local_heads, value_size)
    outgate = outgate_p.reshape(seq_local, local_heads, value_size)
    beta = jax.nn.sigmoid(write_p)
    decay = -jnp.exp(decay_rate)[None, :] * jax.nn.softplus(decay_p)
    kept = state * jnp.exp(decay)[..., None, None]
    seen = jnp.einsum("bhk,bhkv->bhv", keys, kept, precision=lax.Precision.HIGHEST)
    delta = beta[..., None] * (vals - seen)
    new_state = kept + keys[..., :, None] * delta[..., None, :]
    outs = jnp.einsum("bhk,bhkv->bhv", query, new_state, precision=lax.Precision.HIGHEST)
    normed = outs * lax.rsqrt(jnp.mean(outs * outs, -1, keepdims=True) + rms_eps) * norm_gain
    heads_out = (
        (normed * jax.nn.silu(outgate))
        .astype(jnp.bfloat16)
        .reshape(seq_local, local_heads * value_size)
    )
    out_terms = jnp.dot(
        lax.all_gather(heads_out, "kv", axis=0, tiled=True),
        out_weight,
        preferred_element_type=jnp.float32,
    )
    mix = lax.psum_scatter(out_terms.astype(jnp.bfloat16), "tp", scatter_dimension=1, tiled=True)
    second = (residual_scale * mixed_own.astype(jnp.float32) + mix.astype(jnp.float32)).astype(
        jnp.bfloat16
    )
    second = lax.optimization_barrier(second)
    second_rows = lax.all_gather(second, ("kv", "tp"), axis=1, tiled=True)
    mlp_rows = whole_norm(second_rows, layer_gain[1])
    mlp_own = lax.dynamic_slice_in_dim(mlp_rows, own_start, own, 1)
    gate_two = jnp.dot(mlp_rows, gate_second, preferred_element_type=jnp.float32)
    up_two = jnp.dot(mlp_rows, up_second, preferred_element_type=jnp.float32)
    hidden_two = (jax.nn.silu(gate_two) * up_two).astype(jnp.bfloat16)
    terms_two = jnp.dot(hidden_two, down_second, preferred_element_type=jnp.float32)
    branch_two = lax.psum_scatter(terms_two, ("kv", "tp"), scatter_dimension=1, tiled=True)
    third = (residual_scale * mlp_own.astype(jnp.float32) + 0.5 * branch_two).astype(jnp.bfloat16)
    third = lax.optimization_barrier(third)
    gain_two = lax.dynamic_slice_in_dim(layer_gain[2], own_start, own)
    layer_out = spread_norm(third, gain_two, width)
    return (layer_out, new_state)


def dot(a, b):
    return jnp.dot(a, b, preferred_element_type=f32)


def dot_t(a, b):
    return lax.dot_general(a, b, (((1,), (1,)), ((), ())), preferred_element_type=f32)


def silu(x):
    return x * jax.nn.sigmoid(x)


def kernel(
    n_kv,
    n_tp,
    tokens,
    gate_first,
    up_first,
    down_first,
    gate_second,
    up_second,
    down_second,
    query_weight,
    key_weight,
    value_weight,
    outgate_weight,
    decay_weight,
    write_weight,
    decay_rate,
    norm_gain,
    layer_gain,
    out_weight,
    state,
    layer_out,
    new_state,
    tok,
    g1,
    u1,
    d1,
    g2,
    u2,
    d2,
    wq,
    wk,
    wv,
    wo,
    wd,
    ww,
    rate,
    ngain,
    lgain,
    ow,
    st,
    ns,
    out_v,
    red_out,
    red_in,
    red_out2,
    red_in2,
    gain_buf,
    first_buf,
    proj_out,
    proj_in,
    head_buf,
    mix_buf,
    mixed_buf,
    own_block,
    stat2_buf,
    stat_rows,
    load_sem,
    send_sem,
    recv_sem,
):
    n = n_kv * n_tp
    kv = lax.axis_index("kv")
    tp = lax.axis_index("tp")
    me = kv * n_tp + tp
    group, own = tokens.shape
    width = n * own
    block = wq.shape[0]
    seqs, heads, dk, dv = state.shape
    pairs = seqs * heads
    cols = heads * dk
    block_start = pl.multiple_of(kv * block, block)

    loads = {}

    def load(name, src, dst):
        loads[name] = pltpu.make_async_copy(src, dst, load_sem.at[len(loads)])
        loads[name].start()

    load("tok", tokens, tok.at[me])
    load("g1", gate_first, g1)
    load("u1", up_first, u1)
    load("d1", down_first, d1)
    load("lgain", layer_gain, lgain)
    load("wq", query_weight, wq)
    load("wk", key_weight, wk)
    load("wv", value_weight, wv)
    load("wo", outgate_weight, wo)
    load("wd", decay_weight.at[:, pl.ds(block_start, block)], wd)
    load("ww", write_weight.at[:, pl.ds(block_start, block)], ww)
    load("rate", decay_rate, rate)
    load("ngain", norm_gain, ngain)
    load("st", state, st)
    load("ow", out_weight, ow)
    load("g2", gate_second, g2)
    load("u2", up_second, u2)
    load("d2", down_second, d2)

    ring = sorted(range(n_kv), key=lambda d: min(d, n_kv - d))
    near = [(dk, dt) for dk in ring for dt in range(n_tp)]
    partners = [p for p in near if p[0] == 0 and p[1]]
    far = [p for p in near if p[0]][::-1]

    def peer_of(step):
        pk = lax.rem(kv + step[0], n_kv)
        pt = lax.rem(tp + step[1], n_tp)
        return pk * n_tp + pt, pk, pt

    barrier = pltpu.get_barrier_semaphore()
    for step in far + partners:
        _, pk, pt = peer_of(step)
        pl.semaphore_signal(
            barrier,
            inc=1,
            device_id={"kv": pk, "tp": pt},
            device_id_type=pl.DeviceIdType.MESH,
        )
    pl.semaphore_wait(barrier, n - 1)

    sends = []

    def send(kind, src, dst, pk, pt):
        other = pk * n_tp + pt
        copy = pltpu.make_async_remote_copy(
            src_ref=src,
            dst_ref=dst,
            send_sem=send_sem.at[kind, other],
            recv_sem=recv_sem.at[kind, me],
            device_id={"kv": pk, "tp": pt},
            device_id_type=pl.DeviceIdType.MESH,
        )
        copy.start()
        sends.append(copy)

    def receive(kind, dst, pk, pt):
        other = pk * n_tp + pt
        pltpu.make_async_remote_copy(
            src_ref=dst,
            dst_ref=dst,
            send_sem=send_sem.at[kind, other],
            recv_sem=recv_sem.at[kind, other],
            device_id={"kv": pk, "tp": pt},
            device_id_type=pl.DeviceIdType.MESH,
        ).wait_recv()

    def send_all(kind, src_of, dst):
        for step in partners + far:
            other, pk, pt = peer_of(step)
            send(kind, src_of(other), dst, pk, pt)

    def receive_all(kind, buf):
        for step in near[1:]:
            other, pk, pt = peer_of(step)
            receive(kind, buf.at[other], pk, pt)

    def send_kv(kind, src_of, dst):
        for step in ring[:0:-1]:
            pk = lax.rem(kv + step, n_kv)
            send(kind, src_of(pk), dst, pk, tp)

    def receive_kv(kind, buf):
        for step in range(1, n_kv):
            pk = lax.rem(kv + step, n_kv)
            receive(kind, buf.at[pk], pk, tp)

    other_tp = lax.rem(tp + 1, n_tp)

    loads["tok"].wait()
    send_all(TOK, lambda other: tok.at[me], tok.at[me])
    loads["g1"].wait()
    loads["u1"].wait()

    def slot(other):
        return pl.ds(pl.multiple_of(other * own, own), own)

    def send_shares(kind, hidden, dw, send_buf, recv_buf):
        for step in far + partners:
            other, pk, pt = peer_of(step)
            send_buf[other] = dot(hidden, dw[:, slot(other)]).astype(bf16)
            send(kind, send_buf.at[other], recv_buf.at[me], pk, pt)
        recv_buf[me] = dot(hidden, dw[:, slot(me)]).astype(bf16)

    gate, up = 0.0, 0.0
    for step in near:
        other, pk, pt = peer_of(step)
        if step != (0, 0):
            receive(TOK, tok.at[other], pk, pt)
        gate = gate + dot_t(tok[other], g1[:, slot(other)])
        up = up + dot_t(tok[other], u1[:, slot(other)])
    hidden = (silu(gate) * up).astype(bf16)
    loads["d1"].wait()
    send_shares(RED1, hidden, d1, red_out, red_in)

    for name in ("lgain", "wq", "wk", "wv", "wo", "wd", "ww"):
        loads[name].wait()
    gain_block = lgain[0:1, pl.ds(block_start, block)]

    def project(x):
        parts = [dot(x, w[...]) for w in (wq, wk, wv, wo)]
        for w in (wd, ww):
            parts.append(dot_t(x, w[...]))
        return parts

    n_small = wd.shape[0]
    spans = [i * cols for i in range(4)] + [4 * cols, 4 * cols + 128]
    lengths = [cols] * 4 + [n_small] * 2
    gains = project(jnp.broadcast_to(gain_block, (group, block)).astype(bf16))
    gain_buf[kv] = jnp.zeros(gain_buf.shape[1:], f32)
    for part, start, length in zip(gains, spans, lengths):
        gain_buf[kv, :, start : start + length] = part[0:1]
    send_kv(GAINS, lambda pk: gain_buf.at[kv], gain_buf.at[kv])

    receive_all(RED1, red_in)
    branch = red_in[0].astype(f32)
    for s in range(1, n):
        branch = branch + red_in[s].astype(f32)
    first = (residual_scale * tok[me].astype(f32) + 0.5 * branch).astype(bf16)
    first_buf[me] = first
    send_all(FIRST, lambda other: first_buf.at[me], first_buf.at[me])
    for step in partners:
        other, pk, pt = peer_of(step)
        receive(FIRST, first_buf.at[other], pk, pt)
    rows = jnp.concatenate(
        [first_buf[kv * n_tp + t].astype(f32) for t in range(n_tp)], axis=1
    )
    centre = jnp.sum(rows, -1, keepdims=True) / block
    partial = project(((rows - centre) * gain_block).astype(bf16))
    for j in range(n_kv):
        proj_out[j] = jnp.zeros(proj_out.shape[1:], bf16)
        for part, start, length in zip(partial, spans, lengths):
            proj_out[j, :, start : start + length] = part[
                j * seqs : (j + 1) * seqs
            ].astype(bf16)
    send_kv(PROJ, lambda pk: proj_out.at[pk], proj_in.at[kv])
    proj_in[kv] = proj_out[kv]

    for step in near[n_tp:]:
        other, pk, pt = peer_of(step)
        receive(FIRST, first_buf.at[other], pk, pt)
    receive_kv(GAINS, gain_buf)

    def sums(values):
        total = jnp.sum(values, -1, keepdims=True)
        squares = jnp.sum(values * values, -1, keepdims=True)
        return jnp.where(lane == 0, total, jnp.where(lane == 1, squares, 0.0))

    def moments(total, squares):
        mean = total / width
        return mean, lax.rsqrt(squares / width - mean * mean + ln_eps)

    values = [first_buf[s].astype(f32) for s in range(n)]
    totals = [jnp.sum(v, -1, keepdims=True) for v in values]
    squares = sum(jnp.sum(v * v, -1, keepdims=True) for v in values)
    mean, rstd = moments(sum(totals), squares)
    lane = lax.broadcasted_iota(jnp.int32, (group, 128), 1)
    packed = jnp.where(lane == n_kv, rstd, 0.0)
    for j in range(n_kv):
        local = sum(totals[j * n_tp : (j + 1) * n_tp])
        packed = jnp.where(lane == j, local / block - mean, packed)
    stat_rows[...] = packed
    mine = stat_rows[pl.ds(kv * seqs, seqs), :]

    receive_kv(PROJ, proj_in)
    summed = jnp.zeros((seqs, proj_in.shape[2]), f32)
    for j in range(n_kv):
        summed = summed + proj_in[j].astype(f32) + mine[:, j : j + 1] * gain_buf[j]
    summed = (summed * mine[:, n_kv : n_kv + 1]).astype(bf16).astype(f32)

    def by_head(base):
        return jnp.concatenate(
            [
                summed[s : s + 1, base + h * dk : base + (h + 1) * dk]
                for s in range(seqs)
                for h in range(heads)
            ],
            axis=0,
        )

    def unit(values):
        return values * lax.rsqrt(jnp.sum(values * values, -1, keepdims=True) + rms_eps)

    query = unit(silu(by_head(0))) * dk ** (-0.5)
    keys = unit(silu(by_head(cols)))
    vals = silu(by_head(2 * cols))
    outgate = by_head(3 * cols)
    pair_lane = lax.broadcasted_iota(jnp.int32, (pairs, 128), 1)
    pair_head = lax.rem(lax.broadcasted_iota(jnp.int32, (pairs, 128), 0), heads)

    def per_head(base):
        spread = jnp.concatenate(
            [
                jnp.broadcast_to(summed[s : s + 1, base : base + 128], (heads, 128))
                for s in range(seqs)
            ],
            axis=0,
        )
        picked = jnp.where(pair_lane == pair_head + tp * heads, spread, 0.0)
        return jnp.sum(picked, -1, keepdims=True)

    decay_pre = per_head(4 * cols)
    beta = jax.nn.sigmoid(per_head(4 * cols + 128))
    loads["rate"].wait()
    rate_lane = lax.broadcasted_iota(jnp.int32, (pairs, heads), 1)
    rate_head = lax.rem(lax.broadcasted_iota(jnp.int32, (pairs, heads), 0), heads)
    rates = jnp.sum(
        jnp.where(rate_lane == rate_head, jnp.broadcast_to(rate[...], (pairs, heads)), 0.0),
        -1,
        keepdims=True,
    )
    softplus = jnp.maximum(decay_pre, 0.0) + jnp.log1p(jnp.exp(-jnp.abs(decay_pre)))
    factor = jnp.broadcast_to(jnp.exp(-jnp.exp(rates) * softplus), (pairs, dv))
    beta = jnp.broadcast_to(beta, (pairs, dv))
    keys_t = jnp.transpose(keys)
    query_t = jnp.transpose(query)
    loads["st"].wait()
    outs = []
    for s in range(seqs):
        for h in range(heads):
            i = s * heads + h
            kept = st[s, h] * factor[i : i + 1]
            key = keys_t[:, i : i + 1]
            seen = jnp.sum(kept * key, 0, keepdims=True)
            fresh = kept + key * (beta[i : i + 1] * (vals[i : i + 1] - seen))
            ns[s, h] = fresh
            outs.append(jnp.sum(fresh * query_t[:, i : i + 1], 0, keepdims=True))
    outs = jnp.concatenate(outs, axis=0)
    loads["ngain"].wait()
    normed = outs * lax.rsqrt(jnp.mean(outs * outs, -1, keepdims=True) + rms_eps) * ngain[...]
    gated = (normed * silu(outgate)).astype(bf16)
    for s in range(seqs):
        for h in range(heads):
            i = s * heads + h
            head_buf[kv, s : s + 1, h * dv : (h + 1) * dv] = gated[i : i + 1]
    send_kv(HEADS, lambda pk: head_buf.at[kv], head_buf.at[kv])
    store = pltpu.make_async_copy(ns, new_state, load_sem.at[len(loads)])
    store.start()
    for s in range(n):
        scaled = (values[s] - mean) * rstd * lgain[0:1, s * own : (s + 1) * own]
        mixed_buf[s] = scaled.astype(bf16)
    loads["ow"].wait()
    receive_kv(HEADS, head_buf)
    everyone = jnp.concatenate([head_buf[j].astype(f32) for j in range(n_kv)], axis=0)
    mix_buf[me] = dot(everyone.astype(bf16), ow[...]).astype(bf16)
    send_all(MIX, lambda other: mix_buf.at[me], mix_buf.at[me])
    loads["g2"].wait()
    loads["u2"].wait()

    gate, up, total, squares = 0.0, 0.0, 0.0, 0.0
    centre = None
    for hop in ring:
        for dt in range(n_tp):
            other, pk, pt = peer_of((hop, dt))
            if (hop, dt) != (0, 0):
                receive(MIX, mix_buf.at[other], pk, pt)
        pk = lax.rem(kv + hop, n_kv)
        mix = mix_buf[pk * n_tp].astype(f32)
        for t in range(1, n_tp):
            mix = mix + mix_buf[pk * n_tp + t].astype(f32)
        mixed = jnp.concatenate([mixed_buf[pk * n_tp + t] for t in range(n_tp)], axis=1)
        second = residual_scale * mixed.astype(f32) + mix.astype(bf16).astype(f32)
        second = second.astype(bf16).astype(f32)
        sub = jnp.sum(second, -1, keepdims=True)
        if centre is None:
            centre = sub / block
            own_block[...] = second
        total = total + sub
        squares = squares + jnp.sum(second * second, -1, keepdims=True)
        span = pl.ds(pl.multiple_of(pk * block, block), block)
        gain = lgain[1:2, span]
        x = jnp.concatenate(
            [(second - centre) * gain, jnp.broadcast_to(gain, (group, block))], axis=0
        ).astype(bf16)
        gate = gate + dot_t(x, g2[:, span])
        up = up + dot_t(x, u2[:, span])
    mean, rstd = moments(total, squares)
    shift = mean - centre
    gate = rstd * (gate[:group] - shift * gate[group : group + 1])
    up = rstd * (up[:group] - shift * up[group : group + 1])
    hidden = (silu(gate) * up).astype(bf16)
    loads["d2"].wait()
    send_shares(RED2, hidden, d2, red_out2, red_in2)
    second_own = own_block[:, slot(tp)]
    mlp_own = (second_own - mean) * rstd * lgain[1:2, slot(me)]
    mlp_own = mlp_own.astype(bf16).astype(f32)
    receive_all(RED2, red_in2)
    branch = red_in2[0].astype(f32)
    for s in range(1, n):
        branch = branch + red_in2[s].astype(f32)
    third = (residual_scale * mlp_own + 0.5 * branch).astype(bf16).astype(f32)
    stat2_buf[me] = sums(third)
    send_all(STAT2, lambda other: stat2_buf.at[me], stat2_buf.at[me])
    receive_all(STAT2, stat2_buf)
    total = stat2_buf[0]
    for s in range(1, n):
        total = total + stat2_buf[s]
    mean, rstd = moments(total[:, 0:1], total[:, 1:2])
    out_v[...] = ((third - mean) * rstd * lgain[2:3, slot(me)]).astype(bf16)
    final = pltpu.make_async_copy(out_v, layer_out, load_sem.at[len(loads) + 1])
    final.start()
    for copy in sends:
        copy.wait_send()
    store.wait()
    final.wait()


def shards(n_kv, n_tp, *args):
    if args[0].shape[1] % 128 or args[17].shape[2] != 128:
        return shards_by_collectives(*args)
    args = list(args)
    for i in (1, 2, 4, 5, 11, 12):
        args[i] = args[i].T
    args[13] = args[13].reshape(1, -1)
    args[14] = args[14].reshape(1, -1)
    tokens, decay_weight, state = args[0], args[11], args[17]
    query_weight = args[7]
    n = n_kv * n_tp
    group, own = tokens.shape
    seqs = state.shape[0]
    block, cols = query_weight.shape
    small = decay_weight.shape[0]
    flat = 4 * cols + 2 * 128

    def like(x):
        return pltpu.VMEM(x.shape, x.dtype)

    scratch = [
        pltpu.VMEM((n, group, own), bf16),
        *[like(x) for x in args[1:11]],
        pltpu.VMEM((small, block), bf16),
        pltpu.VMEM((small, block), bf16),
        *[like(x) for x in args[13:18]],
        like(state),
        like(tokens),
        pltpu.VMEM((n, group, own), bf16),
        pltpu.VMEM((n, group, own), bf16),
        pltpu.VMEM((n, group, own), bf16),
        pltpu.VMEM((n, group, own), bf16),
        pltpu.VMEM((n_kv, 1, flat), f32),
        pltpu.VMEM((n, group, own), bf16),
        pltpu.VMEM((n_kv, seqs, flat), bf16),
        pltpu.VMEM((n_kv, seqs, flat), bf16),
        pltpu.VMEM((n_kv, seqs, cols), bf16),
        pltpu.VMEM((n, group, n_tp * own), bf16),
        pltpu.VMEM((n, group, own), bf16),
        pltpu.VMEM((group, n_tp * own), f32),
        pltpu.VMEM((n, group, 128), f32),
        pltpu.VMEM((group, 128), f32),
        pltpu.SemaphoreType.DMA((20,)),
        pltpu.SemaphoreType.DMA((9, n)),
        pltpu.SemaphoreType.DMA((9, n)),
    ]
    args = [pltpu.with_memory_space_constraint(a, pltpu.HBM) for a in args]
    return pl.pallas_call(
        functools.partial(kernel, n_kv, n_tp),
        out_shape=(
            jax.ShapeDtypeStruct(tokens.shape, tokens.dtype),
            jax.ShapeDtypeStruct(state.shape, state.dtype),
        ),
        in_specs=[pl.BlockSpec(memory_space=pl.ANY)] * len(args),
        out_specs=(pl.BlockSpec(memory_space=pl.ANY),) * 2,
        scratch_shapes=scratch,
        compiler_params=pltpu.CompilerParams(
            collective_id=0, has_side_effects=True, vmem_limit_bytes=40 * 1024 * 1024
        ),
    )(*args)


def solution(mesh):
    in_specs = (
        P("dp", ("kv", "tp")),
        P(None, ("kv", "tp")),
        P(None, ("kv", "tp")),
        P(("kv", "tp"), None),
        P(None, ("kv", "tp")),
        P(None, ("kv", "tp")),
        P(("kv", "tp"), None),
        P("kv", "tp"),
        P("kv", "tp"),
        P("kv", "tp"),
        P("kv", "tp"),
        P(),
        P(),
        P("tp"),
        P(),
        P(),
        P("tp", "kv"),
        P(("dp", "kv"), "tp", None, None),
    )
    out_specs = (P("dp", ("kv", "tp")), P(("dp", "kv"), "tp", None, None))
    body = functools.partial(shards, mesh.shape["kv"], mesh.shape["tp"])
    return jax.shard_map(body, mesh=mesh, in_specs=in_specs, out_specs=out_specs, check_vma=False)
```
